512 devices in a mesh: fs: 128 (over z, y, core), tp: 4 (over x).
Axes of the slice: x: 4, y: 8, z: 8, core: 2. Of those that a mesh axis runs over, the one named last changes fastest.
Arguments:
- block_input: bfloat16 [24576, 2048], P('fs'), may hold values from -6 to 6
- query_cotangent: bfloat16 [24576, 1024], P('fs', 'tp'), may hold values from -0.0390625 to 0.0390625
- key_cotangent: bfloat16 [24576, 1024], P('fs', 'tp'), may hold values from -0.0390625 to 0.0390625
- query_factor: bfloat16 [2048, 256], P('fs'), may hold values from -0.125 to 0.125
- key_factor: bfloat16 [2048, 256], P('fs'), may hold values from -0.125 to 0.125
- query_first: float32 [256, 1024], P('fs', 'tp'), may hold values from -0.6 to 0.6
- query_second: float32 [256, 1024], P('fs', 'tp'), may hold values from 0.005 to 0.03
- key_first: float32 [256, 1024], P('fs', 'tp'), may hold values from -0.6 to 0.6
- key_second: float32 [256, 1024], P('fs', 'tp'), may hold values from 0.005 to 0.03
- query_weight: float32 [2048, 1024], P('fs', 'tp'), may hold values from -0.125 to 0.125
- key_weight: float32 [2048, 1024], P('fs', 'tp'), may hold values from -0.125 to 0.125
Outputs:
- query_update: float32 [2048, 1024], P('fs', 'tp')
- query_new: float32 [2048, 1024], P('fs', 'tp')
- query_copy: bfloat16 [2048, 1024], P(None, 'tp')
- query_first_new: float32 [256, 1024], P('fs', 'tp')
- query_second_new: float32 [256, 1024], P('fs', 'tp')
- key_update: float32 [2048, 1024], P('fs', 'tp')
- key_new: float32 [2048, 1024], P('fs', 'tp')
- key_copy: bfloat16 [2048, 1024], P(None, 'tp')
- key_first_new: float32 [256, 1024], P('fs', 'tp')
- key_second_new: float32 [256, 1024], P('fs', 'tp')
The draws below stay inside these ranges and needn't reach their ends.
All inputs are finite; a program needn't handle non-finite values.
Results may differ from the reference program's by a relative error of at most 0.0005.
Values may be sent and summed in bfloat16 or wider, within the bound.
A program may use at most 64 MiB of HBM per device.

```python
import math
import jax
import jax.numpy as jnp
from jax import lax

D = 2048
WIDTH = 1024
RANK = 256
TOKENS = 24576


def block_levels(own_key, extent, split, smallest, high):
    def one(axis_at, shards_of):
        steps = jax.random.uniform(jax.random.fold_in(jax.random.fold_in(own_key, 6), axis_at), (shards_of,), jnp.float32, smallest / len(split), high / len(split))
        return jnp.repeat(jnp.exp(steps), extent[axis_at] // shards_of).reshape((-1,) + (1,) * (len(extent) - axis_at - 1))

    loudness = one(*split[0])
    for cut in split[1:]:
        loudness = loudness * one(*cut)
    return loudness


def gaussian(stream_key, shape, width, limit, pieces=(), kind=jnp.bfloat16):
    factor_of = block_levels(stream_key, shape, pieces, -0.22, 0.18) if pieces else 1.0
    array = jax.random.normal(stream_key, shape, jnp.float32) * width * factor_of
    return jnp.minimum(jnp.maximum(array, -limit), limit).astype(kind)


def setup_inputs(seed: int = 0) -> dict:
    keys = jax.random.split(jax.random.key(seed), 12)
    return {
        "block_input": gaussian(keys[0], (TOKENS, D), 1.0, 6.0, ((0, 128),)),
        "query_cotangent": gaussian(keys[1], (TOKENS, WIDTH), TOKENS ** -0.5, 0.0390625, ((0, 128), (1, 4))),
        "key_cotangent": gaussian(keys[2], (TOKENS, WIDTH), TOKENS ** -0.5, 0.0390625, ((0, 128), (1, 4))),
        "query_factor": gaussian(keys[3], (D, RANK), D ** -0.5, 0.125, ((0, 128),)),
        "key_factor": gaussian(keys[4], (D, RANK), D ** -0.5, 0.125, ((0, 128),)),
        "query_first": gaussian(keys[5], (RANK, WIDTH), 0.1, 0.6, ((0, 128), (1, 4)), jnp.float32),
        "query_second": jnp.clip(jnp.exp(math.log(0.03) - 1.7917595 * jax.random.uniform(keys[6], (RANK, WIDTH), jnp.float32) ** block_levels(keys[6], (RANK, WIDTH), ((0, 128), (1, 4)), -0.2, 0.2)), 0.005, 0.03),
        "key_first": gaussian(keys[7], (RANK, WIDTH), 0.1, 0.6, ((0, 128), (1, 4)), jnp.float32),
        "key_second": jnp.clip(jnp.exp(math.log(0.03) - 1.7917595 * jax.random.uniform(keys[8], (RANK, WIDTH), jnp.float32) ** block_levels(keys[8], (RANK, WIDTH), ((0, 128), (1, 4)), -0.2, 0.2)), 0.005, 0.03),
        "query_weight": gaussian(keys[9], (D, WIDTH), D ** -0.5, 0.125, ((0, 128), (1, 4)), jnp.float32),
        "key_weight": gaussian(keys[10], (D, WIDTH), D ** -0.5, 0.125, ((0, 128), (1, 4)), jnp.float32),
    }


beta_one = 0.9
beta_two = 0.99
denom_floor = 0.001
scale_floor = 0.5
learn_rate = 0.02

def one_update(block_input, cotangent, factor, first, second, weight):
    gradient = jnp.dot(block_input.T, cotangent, preferred_element_type=jnp.float32)
    factor_wide = factor.astype(jnp.float32)
    small = jnp.dot(factor_wide.T, gradient, precision=lax.Precision.HIGHEST)
    first_new = beta_one * first + (1.0 - beta_one) * small
    second_new = beta_two * second + (1.0 - beta_two) * small * small
    direction = first_new / (jnp.sqrt(second_new) + denom_floor)
    spread = jnp.sqrt(jnp.sum(direction * direction) / direction.size)
    scale = 1.0 / jnp.maximum(spread, scale_floor)
    update = -scale * jnp.dot(factor_wide, direction, precision=lax.Precision.HIGHEST)
    fresh = weight + learn_rate * update
    return (update, fresh, fresh.astype(jnp.bfloat16), first_new, second_new)

def reference(block_input, query_cotangent, key_cotangent, query_factor, key_factor, query_first, query_second, key_first, key_second, query_weight, key_weight):
    query_out = one_update(block_input, query_cotangent, query_factor, query_first, query_second, query_weight)
    key_out = one_update(block_input, key_cotangent, key_factor, key_first, key_second, key_weight)
    return (query_out[0], query_out[1], query_out[2], query_out[3], query_out[4], key_out[0], key_out[1], key_out[2], key_out[3], key_out[4])
```

```python
import functools

import jax
import jax.numpy as jnp
from jax import lax
from jax.experimental import pallas as pl
from jax.experimental.pallas import tpu as pltpu
from jax.sharding import Mesh
from jax.sharding import PartitionSpec as P

MESH = pl.DeviceIdType.MESH
FS = ("z", "y", "c")
N = 8
SUBS = 4
FAR_FIRST = (4, 3, 5, 2, 6, 1, 7)
NEAR_FIRST = (1, 7, 2, 6, 3, 5, 4)

beta_one = 0.9
beta_two = 0.99
denom_floor = 0.001
scale_floor = 0.5
learn_rate = 0.02

f32 = jnp.float32
bf16 = jnp.bfloat16


def two_pieces(v):
    high = v.astype(bf16)
    low = (v - high.astype(f32)).astype(bf16)
    return high, low


class Part:
    def __init__(self, first, second, pos):
        self.first, self.second = first, second
        self.f, self.s, self.c = pos[first], pos[second], pos["c"]
        self.rows_second = second == "z"

    def block(self, buf, f, s, c):
        if self.rows_second:
            return buf.at[s, f // 2, f % 2, c]
        return buf.at[f // 2, f % 2, s, c]

    def sub(self, buf, j, s, c):
        if self.rows_second:
            return buf.at[s, j, :, c]
        return buf.at[j, :, s, c]

    def half(self, buf, h, s, c):
        if self.rows_second:
            return buf.at[s, pl.ds(2 * h, 2), :, c]
        return buf.at[pl.ds(2 * h, 2), :, s, c]

    def strip(self, buf, s, c):
        if self.rows_second:
            return buf.at[s, :, :, c]
        return buf.at[:, :, s, c]


def rows_of(buf, k, b):
    return (buf[b] if k == 0 else buf[b // 2, b % 2]).reshape(256, 256)


def own_rows(buf, k, z, y, c):
    return buf[z, y // 2, y % 2, c] if k == 0 else buf[z // 2, z % 2, y, c]


def ring(v, d):
    return lax.rem(v + (d + 2 * N), N)


class Sends:
    def __init__(self, sems):
        self.sems, self.used, self.open = sems, 0, []

    def __call__(self, src, dst, recv, to):
        copy = pltpu.make_async_remote_copy(
            src_ref=src,
            dst_ref=dst,
            send_sem=self.sems.at[self.used],
            recv_sem=recv,
            device_id=to,
            device_id_type=MESH,
        )
        self.used += 1
        copy.start()
        self.open.append(copy)

    def arrived(self, ref, recv, to):
        pltpu.make_async_remote_copy(
            src_ref=ref, dst_ref=ref, send_sem=self.sems.at[0], recv_sem=recv, device_id=to, device_id_type=MESH
        ).wait_recv()

    def finish(self):
        for copy in self.open:
            copy.wait_send()


def exchange_kernel(
    x_hbm, cq_hbm, ck_hbm, fq_hbm, fk_hbm, q1_hbm, q2_hbm, k1_hbm, k2_hbm, wq_hbm, wk_hbm,
    FQ, FK, WQ, WK, DQ, DK, total_ref, mom_ref,
    xv, cqv, ckv, fown, MQ, MK, MF, PB, PR, SB, R1, S1, R2, SS, T, M8,
    loc, send_sems, d1, rr, rl, dd, w1, wr, wl, wd, ms, ps, b1, b2, c1, cd, xs,
):
    pos = {a: lax.axis_index(a) for a in ("z", "y", "c")}
    me_x = lax.axis_index("tp")
    z, y, c = pos["z"], pos["y"], pos["c"]
    query, key = Part("y", "z", pos), Part("z", "y", pos)
    parts = (query, key)
    F, W, Dn, Mo = (FQ, FK), (WQ, WK), (DQ, DK), (MQ, MK)
    other = {"c": 1 - c}

    loads = []

    def load(src, dst):
        copy = pltpu.make_async_copy(src, dst, loc.at[len(loads)])
        copy.start()
        loads.append(copy)

    load(fq_hbm, fown.at[0])
    load(fk_hbm, fown.at[1])
    load(q1_hbm, MQ.at[z, 0])
    load(q2_hbm, MQ.at[z, 1])
    load(k1_hbm, MK.at[y, 0])
    load(k2_hbm, MK.at[y, 1])
    load(wq_hbm, query.block(WQ, query.f, query.s, c))
    load(wk_hbm, key.block(WK, key.f, key.s, c))
    load(cq_hbm, cqv)
    load(ck_hbm, ckv)
    load(x_hbm, xv)

    barrier = pltpu.get_barrier_semaphore()
    for d in range(1, N):
        pl.semaphore_signal(barrier, inc=1, device_id={"y": ring(y, d)}, device_id_type=MESH)
        pl.semaphore_signal(barrier, inc=1, device_id={"z": ring(z, d)}, device_id_type=MESH)
    pl.semaphore_signal(barrier, inc=1, device_id=other, device_id_type=MESH)
    for d in range(1, 4):
        pl.semaphore_signal(barrier, inc=1, device_id={"tp": lax.rem(me_x + d, 4)}, device_id_type=MESH)

    rank = lax.broadcasted_iota(jnp.int32, (256, 256), 0)
    slot = lax.broadcasted_iota(jnp.int32, (256, 256), 1)
    sf, sc, ss, si = slot >> 5, (slot >> 4) & 1, (slot >> 1) & 7, slot & 1
    places = (((ss * 8 + sf) * 2 + sc) * 2 + si, ((sf * 8 + ss) * 2 + sc) * 2 + si)
    loads[0].wait()
    loads[1].wait()
    for k, part in enumerate(parts):
        order = jnp.where(rank == places[k], 1.0, 0.0).astype(bf16)
        mine = jnp.dot(fown[k], order, preferred_element_type=f32).astype(bf16)
        part.block(F[k], part.f, part.s, c)[...] = mine

    for copy in loads[2:8]:
        copy.wait()
    pl.semaphore_wait(barrier, 2 * (N - 1) + 1 + 3)

    send = Sends(send_sems)

    def direct(k, buf, sems):
        part = parts[k]
        for d in FAR_FIRST:
            mine = part.block(buf, part.f, part.s, c)
            send(mine, mine, sems.at[k, d], {part.first: ring(part.f, d)})

    for k in (0, 1):
        direct(k, F[k], d1)

    def piece(k, t):
        return lax.rem(parts[k].f // 2 + t, SUBS)

    for t in range(4):
        for n in range(SUBS):
            for k, part in enumerate(parts):
                j = piece(k, n)
                right, left = {part.second: ring(part.s, 1)}, {part.second: ring(part.s, -1)}
                if t == 0:
                    for r in (0, 1):
                        fr = 2 * j + r
                        far = lax.rem(part.f - fr + N, N)

                        @pl.when(far != 0)
                        def _():
                            send.arrived(part.block(F[k], fr, part.s, c), d1.at[k, far], other)

                    mine = part.sub(F[k], j, part.s, c)
                    send(mine, mine, rr.at[k, 0, n], right)
                    send(mine, mine, rl.at[k, 0, n], left)
                else:
                    from_left = part.sub(F[k], j, ring(part.s, -t), c)
                    send.arrived(from_left, rr.at[k, t - 1, n], other)
                    if t < 3 or n < SUBS // 2:
                        send(from_left, from_left, rr.at[k, t, n], right)
                    from_right = part.sub(F[k], j, ring(part.s, t), c)
                    send.arrived(from_right, rl.at[k, t - 1, n], other)
                    if t < 3 or n >= SUBS // 2:
                        send(from_right, from_right, rl.at[k, t, n], left)
        for k, part in enumerate(parts):
            for s in [0] if t == 0 else [-t, t]:
                strip = part.strip(F[k], ring(part.s, s), c)
                send(strip, strip, dd.at[k, s + 3], other)
    for k, part in enumerate(parts):
        for n in range(SUBS):
            sems = rr if n < SUBS // 2 else rl
            send.arrived(part.sub(F[k], piece(k, n), ring(part.s, 4), c), sems.at[k, 3, n], other)
        strip = part.strip(F[k], ring(part.s, 4), c)
        send(strip, strip, dd.at[k, 7], other)

    for k, part in enumerate(parts):
        for d in FAR_FIRST:
            mine = Mo[k].at[part.s]
            send(mine, mine, ms.at[k, d], {part.second: ring(part.s, d)})
    for k in (0, 1):
        direct(k, W[k], w1)

    def weights_step(t):
        for k, part in enumerate(parts):
            right, left = {part.second: ring(part.s, 1)}, {part.second: ring(part.s, -1)}
            if t == 0:
                for d in NEAR_FIRST:
                    send.arrived(part.block(W[k], ring(part.f, -d), part.s, c), w1.at[k, d], other)
                mine = part.strip(W[k], part.s, c)
                send(mine, mine, wr.at[k, 0], right)
                send(mine, mine, wl.at[k, 0], left)
                send(mine, mine, wd.at[k, 3], other)
                continue
            if t < 4:
                from_left = part.strip(W[k], ring(part.s, -t), c)
                send.arrived(from_left, wr.at[k, t - 1], other)
                from_right = part.strip(W[k], ring(part.s, t), c)
                send.arrived(from_right, wl.at[k, t - 1], other)
                if t < 3:
                    send(from_left, from_left, wr.at[k, t], right)
                    send(from_right, from_right, wl.at[k, t], left)
                else:
                    low = part.half(W[k], 0, ring(part.s, -3), c)
                    send(low, low, wr.at[k, 3], right)
                    high = part.half(W[k], 1, ring(part.s, 3), c)
                    send(high, high, wl.at[k, 3], left)
                send(from_left, from_left, wd.at[k, 3 - t], other)
                send(from_right, from_right, wd.at[k, 3 + t], other)
                continue
            send.arrived(part.half(W[k], 0, ring(part.s, 4), c), wr.at[k, 3], other)
            send.arrived(part.half(W[k], 1, ring(part.s, 4), c), wl.at[k, 3], other)
            last = part.strip(W[k], ring(part.s, 4), c)
            send(last, last, wd.at[k, 7], other)

    for copy in loads[8:]:
        copy.wait()
    for k, part in enumerate(parts):
        for s in (0, -1, 1, -2, 2, -3, 3, 4):
            send.arrived(
                part.strip(F[k], ring(part.s, s), 1 - c), dd.at[k, s + 3], other
            )
        mixed = jnp.zeros((192, 256), f32)
        for b in range(N):
            block = rows_of(F[k], k, b)
            mixed += jnp.dot(xv[:, b * 256 : (b + 1) * 256], block, preferred_element_type=f32)
        cot = (cqv, ckv)[k][...]
        high, low = two_pieces(mixed)
        product = jnp.dot(high.T, cot, preferred_element_type=f32)
        product += jnp.dot(low.T, cot, preferred_element_type=f32)
        PB[k] = product.reshape(N, 2, 16, 256)
        half = PB.at[k, :, 1 - c]
        send(half, PR.at[k], ps.at[k], other)
    weights_step(0)

    for k, part in enumerate(parts):
        send.arrived(PR.at[k], ps.at[k], other)
        SB[k] = PB[k, :, c] + PR[k]
        for d in FAR_FIRST:
            to = ring(part.f, d)
            send(SB.at[k, to], R1.at[k, part.f], b1.at[k, d], {part.first: to})
    weights_step(1)
    for k, part in enumerate(parts):
        acc = SB[k, part.f]
        for d in NEAR_FIRST:
            src = ring(part.f, -d)
            send.arrived(R1.at[k, src], b1.at[k, d], other)
            acc += R1[k, src]
        R2[k, part.s] = acc
        for d in FAR_FIRST:
            mine = R2.at[k, part.s]
            send(mine, mine, b2.at[k, d], {part.second: ring(part.s, d)})
    for k, part in enumerate(parts):
        for d in NEAR_FIRST:
            src = ring(part.s, -d)
            send.arrived(Mo[k].at[src], ms.at[k, d], other)
        for b in range(N):
            for m in (0, 1):
                MF[k, m, 2 * b : 2 * b + 2, :] = Mo[k][b, m]
    weights_step(2)

    for k, part in enumerate(parts):
        for d in NEAR_FIRST:
            send.arrived(R2.at[k, ring(part.s, -d)], b2.at[k, d], other)
        small = R2[k, 0]
        for b in range(1, N):
            small += R2[k, b]
        first_new = beta_one * MF[k, 0] + (1.0 - beta_one) * small
        second_new = beta_two * MF[k, 1] + (1.0 - beta_two) * small * small
        Dn[k][part.f, c] = first_new / (jnp.sqrt(second_new) + denom_floor)
        for d in FAR_FIRST:
            mine = Dn[k].at[part.f, c]
            send(mine, mine, c1.at[k, d], {part.first: ring(part.f, d)})
        T[k, 0] = first_new
        T[k, 1] = second_new
    weights_step(3)
    for k, part in enumerate(parts):
        for m in (0, 1):
            for b in range(N):
                M8[k, m, b] = T[k, m, 2 * b : 2 * b + 2, :]
            mom_ref[k, m] = M8[k, m, part.s]
    for k, part in enumerate(parts):
        for d in NEAR_FIRST:
            send.arrived(Dn[k].at[ring(part.f, -d), c], c1.at[k, d], other)
        mine = Dn[k].at[:, c]
        send(mine, mine, cd.at[k], other)
    weights_step(4)
    sums = []
    for k, part in enumerate(parts):
        send.arrived(Dn[k].at[:, 1 - c], cd.at[k], other)
        full = Dn[k][...].reshape(256, 256)
        sums.append(jnp.sum(full * full, axis=(0, 1), keepdims=True))
    row = lax.broadcasted_iota(jnp.int32, (8, 256), 0)
    SS[me_x] = jnp.where(row == 0, sums[0], sums[1])
    for d in range(1, 4):
        mine = SS.at[me_x]
        send(mine, mine, xs.at[d], {"tp": lax.rem(me_x + d, 4)})
    for k, part in enumerate(parts):
        for s in (0, -1, 1, -2, 2, -3, 3, 4):
            send.arrived(part.strip(W[k], ring(part.s, s), 1 - c), wd.at[k, s + 3], other)
    for d in range(1, 4):
        send.arrived(SS.at[lax.rem(me_x + 4 - d, 4)], xs.at[d], other)
    total_ref[...] = ((SS[0] + SS[1]) + SS[2]) + SS[3]
    send.finish()


def update_kernel(
    FQ, FK, WQ, WK, DQ, DK, total_ref, mom_ref,
    uq_out, nq_out, cq_out, f1q_out, f2q_out, uk_out, nk_out, ck_out, f1k_out, f2k_out,
    copies, own, mom, sems, small_sems,
):
    z, y, c = (lax.axis_index(a) for a in FS)
    F, W, Dn = (FQ, FK), (WQ, WK), (DQ, DK)
    outs = ((uq_out, nq_out, cq_out, f1q_out, f2q_out), (uk_out, nk_out, ck_out, f1k_out, f2k_out))
    flight = []
    mom[...] = mom_ref[...]
    for k in (0, 1):
        for m in (0, 1):
            copy = pltpu.make_async_copy(mom.at[k, m], outs[k][3 + m], small_sems.at[k, m])
            copy.start()
            flight.append(copy)
    for k in (0, 1):
        total = total_ref[k : k + 1, :]
        scale = 1.0 / jnp.maximum(jnp.sqrt(total * (1.0 / 262144.0)), scale_floor)
        high, low = two_pieces(Dn[k][...].reshape(256, 256))

        def update_of(rows):
            whole = jnp.dot(rows, high, preferred_element_type=f32) + jnp.dot(rows, low, preferred_element_type=f32)
            return -scale * whole

        for b in range(N):
            update = update_of(rows_of(F[k], k, b))
            new = rows_of(W[k], k, b) + learn_rate * update
            copies[k, b] = new.astype(bf16)
            copy = pltpu.make_async_copy(copies.at[k, b], outs[k][2].at[pl.ds(b * 256, 256), :], sems.at[k, b])
            copy.start()
            flight.append(copy)
        update = update_of(own_rows(F[k], k, z, y, c))
        own[k, 0] = update
        own[k, 1] = own_rows(W[k], k, z, y, c) + learn_rate * update
        for m in (0, 1):
            copy = pltpu.make_async_copy(own.at[k, m], outs[k][m], small_sems.at[k, 2 + m])
            copy.start()
            flight.append(copy)
    for copy in flight:
        copy.wait()


def body(block_input, query_cotangent, key_cotangent, query_factor, key_factor,
         query_first, query_second, key_first, key_second, query_weight, key_weight):
    any_spec = pl.BlockSpec(memory_space=pl.ANY)
    vmem = pl.BlockSpec(memory_space=pltpu.VMEM)
    shape = jax.ShapeDtypeStruct
    by_z, by_y = (8, 4, 2, 2, 16, 256), (4, 2, 8, 2, 16, 256)
    dma = pltpu.SemaphoreType.DMA
    mid = pl.pallas_call(
        exchange_kernel,
        out_shape=(
            pltpu.VMEM(by_z, bf16), pltpu.VMEM(by_y, bf16), pltpu.VMEM(by_z, f32), pltpu.VMEM(by_y, f32),
            pltpu.VMEM((8, 2, 16, 256), f32), pltpu.VMEM((8, 2, 16, 256), f32),
            pltpu.VMEM((8, 256), f32), pltpu.VMEM((2, 2, 2, 256), f32),
        ),
        in_specs=[any_spec] * 11,
        out_specs=(vmem,) * 8,
        scratch_shapes=[
            pltpu.VMEM((192, 2048), bf16), pltpu.VMEM((192, 256), bf16), pltpu.VMEM((192, 256), bf16),
            pltpu.VMEM((2, 16, 256), bf16),
            pltpu.VMEM((8, 2, 2, 256), f32), pltpu.VMEM((8, 2, 2, 256), f32), pltpu.VMEM((2, 2, 16, 256), f32),
            pltpu.VMEM((2, 8, 2, 16, 256), f32), pltpu.VMEM((2, 8, 16, 256), f32), pltpu.VMEM((2, 8, 16, 256), f32),
            pltpu.VMEM((2, 8, 16, 256), f32), pltpu.VMEM((8, 256), f32), pltpu.VMEM((2, 8, 16, 256), f32),
            pltpu.VMEM((4, 8, 256), f32), pltpu.VMEM((2, 2, 16, 256), f32), pltpu.VMEM((2, 2, 8, 2, 256), f32),
            dma((11,)), dma((220,)),
            dma((2, 8)), dma((2, 4, 4)), dma((2, 4, 4)), dma((2, 8)),
            dma((2, 8)), dma((2, 4)), dma((2, 4)), dma((2, 8)),
            dma((2, 8)), dma((2,)), dma((2, 8)), dma((2, 8)), dma((2, 8)), dma((2,)), dma((4,)),
        ],
        compiler_params=pltpu.CompilerParams(collective_id=0, has_side_effects=True, vmem_limit_bytes=40 * 1024 * 1024),
    )(block_input, query_cotangent, key_cotangent, query_factor, key_factor,
      query_first, query_second, key_first, key_second, query_weight, key_weight)
    one = (
        shape((16, 256), f32), shape((16, 256), f32), shape((2048, 256), bf16), shape((2, 256), f32), shape((2, 256), f32),
    )
    return pl.pallas_call(
        update_kernel,
        out_shape=one + one,
        in_specs=[vmem] * 8,
        out_specs=(any_spec,) * 10,
        scratch_shapes=[
            pltpu.VMEM((2, 8, 256, 256), bf16), pltpu.VMEM((2, 2, 16, 256), f32), pltpu.VMEM((2, 2, 2, 256), f32),
            dma((2, 8)), dma((2, 4)),
        ],
        compiler_params=pltpu.CompilerParams(vmem_limit_bytes=40 * 1024 * 1024),
    )(*mid)


def solution(mesh):
    split = Mesh(mesh.devices.reshape(8, 8, 2, mesh.shape["tp"]), ("z", "y", "c", "tp"))
    rows, both = P(FS, None), P(FS, "tp")
    one = (both, both, P(None, "tp"), both, both)
    return jax.shard_map(
        body,
        mesh=split,
        in_specs=(rows, both, both, rows, rows, both, both, both, both, both, both),
        out_specs=one + one,
        check_vma=False,
    )
```

```python
import jax
import jax.numpy as jnp
from jax import lax
from jax.experimental import pallas as pl
from jax.experimental.pallas import tpu as pltpu
from jax.sharding import Mesh
from jax.sharding import PartitionSpec as P

MESH = pl.DeviceIdType.MESH
FS = ("z", "y", "c")
N = 8
SUBS = 4
FAR_FIRST = (4, 3, 5, 2, 6, 1, 7)

beta_one = 0.9
beta_two = 0.99
denom_floor = 0.001
scale_floor = 0.5
learn_rate = 0.02

f32 = jnp.float32
bf16 = jnp.bfloat16


def two_pieces(v):
    high = v.astype(bf16)
    low = (v - high.astype(f32)).astype(bf16)
    return high, low


def ring(v, d):
    return lax.rem(v + (d + 2 * N), N)


class Part:
    def __init__(self, first, second, pos):
        self.first, self.second = first, second
        self.f, self.s, self.c = pos[first], pos[second], pos["c"]
        self.by_z = second == "z"

    def block(self, buf, f, s, c):
        return buf.at[s, f // 2, f % 2, c] if self.by_z else buf.at[f // 2, f % 2, s, c]

    def sub(self, buf, j, s, c):
        return buf.at[s, j, :, c] if self.by_z else buf.at[j, :, s, c]

    def half(self, buf, h, s, c):
        return buf.at[s, pl.ds(2 * h, 2), :, c] if self.by_z else buf.at[pl.ds(2 * h, 2), :, s, c]

    def strip(self, buf, s, c):
        return buf.at[s, :, :, c] if self.by_z else buf.at[:, :, s, c]

    def one_core(self, buf):
        return buf.at[:, :, :, 0]

    def peer(self, axis, d):
        return {axis: ring(self.f if axis == self.first else self.s, d)}


def rows_of(buf, k, b):
    return (buf[b] if k == 0 else buf[b // 2, b % 2]).reshape(256, 256)


def own_rows(buf, k, z, y, c):
    return buf[z, y // 2, y % 2, c] if k == 0 else buf[z // 2, z % 2, y, c]


def exchange_kernel(
    x_hbm, cq_hbm, ck_hbm, fq_hbm, fk_hbm, q1_hbm, q2_hbm, k1_hbm, k2_hbm, wq_hbm, wk_hbm,
    FQ, FK, WQ, WK, DQ, DK, total_ref, mom_ref,
    xv, cots, fown, MQ, MK, MF, PB, PR, SB, R1, R2, SX, TT, T, M8,
    loc, out, d1, r2, dd, w1, wr, wl, wd, ms, ps, b1, b2, c1, cd, xs, ts,
):
    pos = {a: lax.axis_index(a) for a in FS}
    x = lax.axis_index("tp")
    z, y, c = pos["z"], pos["y"], pos["c"]
    parts = (Part("y", "z", pos), Part("z", "y", pos))
    both = tuple(enumerate(parts))
    F, W, Dn, Mo = (FQ, FK), (WQ, WK), (DQ, DK), (MQ, MK)
    other = {"c": 1 - c}

    def send(src, dst, group, recv, to):
        pltpu.make_async_remote_copy(
            src_ref=src, dst_ref=dst, send_sem=out.at[group], recv_sem=recv, device_id=to, device_id_type=MESH
        ).start()

    def arrived(view, recv):
        pltpu.make_async_copy(view, view, recv).wait()

    def load(src, dst, sem):
        pltpu.make_async_copy(src, dst, loc.at[sem]).start()

    load(fq_hbm, fown.at[0], 0)
    load(fk_hbm, fown.at[1], 0)
    load(q1_hbm, MQ.at[z, 0], 1)
    load(q2_hbm, MQ.at[z, 1], 1)
    load(k1_hbm, MK.at[y, 0], 2)
    load(k2_hbm, MK.at[y, 1], 2)
    load(wq_hbm, parts[0].block(WQ, y, z, c), 3)
    load(wk_hbm, parts[1].block(WK, z, y, c), 3)
    load(cq_hbm, cots.at[0], 4)
    load(ck_hbm, cots.at[1], 4)
    load(x_hbm, xv, 5)

    barrier = pltpu.get_barrier_semaphore()
    greeted = [{"y": ring(y, d)} for d in range(1, N)] + [{"z": ring(z, d)} for d in range(1, N)] + [other]
    kin = []
    for d in range(1, 4):
        kin += [{"tp": lax.rem(x + d, 4)}, {"tp": lax.rem(x + d, 4), "c": 1 - c}]
    for to in greeted + kin:
        pl.semaphore_signal(barrier, inc=1, device_id=to, device_id_type=MESH)

    rank = lax.broadcasted_iota(jnp.int32, (256, 256), 0)
    slot = lax.broadcasted_iota(jnp.int32, (256, 256), 1)
    sf, sc, ss, si = slot >> 5, (slot >> 4) & 1, (slot >> 1) & 7, slot & 1
    places = (((ss * 8 + sf) * 2 + sc) * 2 + si, ((sf * 8 + ss) * 2 + sc) * 2 + si)
    arrived(fown, loc.at[0])
    for k, p in both:
        order = jnp.where(rank == places[k], 1.0, 0.0).astype(bf16)
        mine = jnp.dot(fown[k], order, preferred_element_type=f32).astype(bf16)
        p.block(F[k], p.f, p.s, c)[...] = mine
    arrived(MQ.at[0], loc.at[1])
    arrived(MK.at[0], loc.at[2])
    arrived(WQ.at[0, 0, :, 0], loc.at[3])
    pl.semaphore_wait(barrier, len(greeted) + len(kin))

    def direct(k, buf, group, recv_of):
        p = parts[k]
        mine = p.block(buf, p.f, p.s, c)
        for d in FAR_FIRST:
            send(mine, mine, group, recv_of(k, p, d), p.peer(p.first, d))

    def pair_sem(k, p, d):
        return d1.at[k, lax.rem(p.f // 2 - ring(p.f, d) // 2 + SUBS, SUBS)]

    for k in (0, 1):
        direct(k, F[k], 0, pair_sem)

    def piece(p, n):
        return lax.rem(p.f // 2 + n, SUBS)

    for n in range(SUBS):
        for k, p in both:
            j = piece(p, n)
            mine = p.sub(F[k], j, p.s, c)
            arrived(p.block(F[k], 0, 0, 0) if n == 0 else mine, d1.at[k, n])
            for d in (2, -2, 1, -1):
                send(mine, mine, 1, r2.at[k, d + 3, n // 2], p.peer(p.second, d))
    for k, p in both:
        mine = p.strip(F[k], p.s, c)
        send(mine, mine, 2, dd.at[k], other)
    for h in (0, 1):
        for k, p in both:
            for way in (1, -1):
                src = ring(p.s, -2 * way)
                arrived(p.half(F[k], 0, src, c), r2.at[k, 2 * way + 3, h])
                for n in (2 * h, 2 * h + 1):
                    got = p.sub(F[k], piece(p, n), src, c)
                    if (h == 0) == (way == 1):
                        send(got, got, 1, r2.at[k, 7, h], p.peer(p.second, 2 * way))
                    send(got, got, 1, r2.at[k, 3 * way + 3, h], p.peer(p.second, way))
    for k, p in both:
        for d in (1, -1):
            for h in (0, 1):
                arrived(p.half(F[k], 0, p.s, c), r2.at[k, d + 3, h])
        for d in (1, -1, 2, -2):
            got = p.strip(F[k], ring(p.s, d), c)
            send(got, got, 2, dd.at[k], other)

    for k, p in both:
        for d in FAR_FIRST:
            mine = Mo[k].at[p.s]
            send(mine, mine, 3 + k, ms.at[k], p.peer(p.second, d))
    for k in (0, 1):
        direct(k, W[k], 5, lambda k, p, d: w1.at[k])

    for k, p in both:
        for d in (3, -3, 4):
            for h in (0, 1):
                arrived(p.half(F[k], 0, p.s, c), r2.at[k, d + 3, h])
            got = p.strip(F[k], ring(p.s, -d), c)
            send(got, got, 2, dd.at[k], other)

    def weights_step(t):
        for k, p in both:
            right, left = p.peer(p.second, 1), p.peer(p.second, -1)
            if t == 0:
                arrived((WQ.at[pl.ds(0, 7), 0, 0, 0]), w1.at[k])
                mine = p.strip(W[k], p.s, c)
                send(mine, mine, 6, wr.at[k, 0], right)
                send(mine, mine, 6, wl.at[k, 0], left)
                send(mine, mine, 7, wd.at[k], other)
            elif t < 4:
                from_left = p.strip(W[k], ring(p.s, -t), c)
                arrived(from_left, wr.at[k, t - 1])
                from_right = p.strip(W[k], ring(p.s, t), c)
                arrived(from_right, wl.at[k, t - 1])
                if t < 3:
                    send(from_left, from_left, 6, wr.at[k, t], right)
                    send(from_right, from_right, 6, wl.at[k, t], left)
                else:
                    low, high = p.half(W[k], 0, ring(p.s, -3), c), p.half(W[k], 1, ring(p.s, 3), c)
                    send(low, low, 6, wr.at[k, 3], right)
                    send(high, high, 6, wl.at[k, 3], left)
                send(from_left, from_left, 7, wd.at[k], other)
                send(from_right, from_right, 7, wd.at[k], other)
            else:
                arrived(p.half(W[k], 0, ring(p.s, 4), c), wr.at[k, 3])
                arrived(p.half(W[k], 1, ring(p.s, 4), c), wl.at[k, 3])
                last = p.strip(W[k], ring(p.s, 4), c)
                send(last, last, 7, wd.at[k], other)

    arrived(cots, loc.at[4])
    arrived(xv, loc.at[5])
    for k, p in both:
        arrived(p.one_core(F[k]), dd.at[k])
        mixed = jnp.zeros((192, 256), f32)
        for b in range(N):
            mixed += jnp.dot(xv[:, b * 256 : (b + 1) * 256], rows_of(F[k], k, b), preferred_element_type=f32)
        high, low = two_pieces(mixed)
        product = jnp.dot(high.T, cots[k], preferred_element_type=f32)
        product += jnp.dot(low.T, cots[k], preferred_element_type=f32)
        PB[k] = product.reshape(N, 2, 16, 256)
        send(PB.at[k, :, 1 - c], PR.at[k], 8, ps.at[k], other)
    weights_step(0)

    for k, p in both:
        arrived(PR.at[k], ps.at[k])
        SB[k] = PB[k, :, c] + PR[k]
        for d in FAR_FIRST:
            to = ring(p.f, d)
            send(SB.at[k, to], R1.at[k, p.f], 9, b1.at[k], {p.first: to})
    weights_step(1)
    for k, p in both:
        arrived(R1.at[k, pl.ds(0, 7)], b1.at[k])
        acc = SB[k, p.f]
        for d in FAR_FIRST:
            acc += R1[k, ring(p.f, -d)]
        R2[k, p.s] = acc
        for d in FAR_FIRST:
            mine = R2.at[k, p.s]
            send(mine, mine, 10, b2.at[k], p.peer(p.second, d))
    for k, p in both:
        arrived(Mo[k].at[pl.ds(0, 7)], ms.at[k])
        for b in range(N):
            for m in (0, 1):
                MF[k, m, 2 * b : 2 * b + 2, :] = Mo[k][b, m]
    weights_step(2)

    sums = []
    for k, p in both:
        arrived(R2.at[k, pl.ds(0, 7)], b2.at[k])
        small = R2[k, 0]
        for b in range(1, N):
            small += R2[k, b]
        first_new = beta_one * MF[k, 0] + (1.0 - beta_one) * small
        second_new = beta_two * MF[k, 1] + (1.0 - beta_two) * small * small
        direction = first_new / (jnp.sqrt(second_new) + denom_floor)
        Dn[k][p.f, c] = direction
        for d in FAR_FIRST:
            mine = Dn[k].at[p.f, c]
            send(mine, mine, 11, c1.at[k], p.peer(p.first, d))
        sums.append(jnp.sum(direction * direction, axis=(0, 1), keepdims=True))
        T[k, 0] = first_new
        T[k, 1] = second_new

    row = lax.broadcasted_iota(jnp.int32, (2, 128), 0)
    SX[2 * x + c] = jnp.where(row == 0, sums[0], sums[1])
    for to in [other] + kin:
        mine = SX.at[2 * x + c]
        send(mine, mine, 13, xs.at[0], to)
    for k, p in both:
        for m in (0, 1):
            for b in range(N):
                M8[k, m, b] = T[k, m, 2 * b : 2 * b + 2, :]
            mom_ref[k, m] = M8[k, m, p.s]
    arrived(SX.at[pl.ds(0, 7)], xs.at[0])
    across = SX[0]
    for b in range(1, N):
        across += SX[b]
    for k, p in both:
        TT[k, p.f] = across
        for d in FAR_FIRST:
            mine = TT.at[k, p.f]
            send(mine, mine, 14, ts.at[k], p.peer(p.first, d))
    weights_step(3)
    for k, p in both:
        arrived(DQ.at[pl.ds(0, 7), 0], c1.at[k])
        mine = Dn[k].at[:, c]
        send(mine, mine, 12, cd.at[k], other)
    weights_step(4)
    totals = []
    for k in (0, 1):
        arrived(TT.at[k, pl.ds(0, 7)], ts.at[k])
        total = TT[k, 0]
        for b in range(1, N):
            total += TT[k, b]
        totals.append(total[k : k + 1, 0:1])
    lane = lax.broadcasted_iota(jnp.int32, (8, 256), 0)
    total_ref[...] = jnp.where(lane == 0, totals[0], totals[1])
    for k, p in both:
        arrived(DQ.at[:, 0], cd.at[k])
        arrived(p.one_core(W[k]), wd.at[k])

    arrived(FQ.at[pl.ds(0, 7), 0, :, 0], out.at[0])
    arrived(FQ.at[pl.ds(0, 7)], out.at[1])
    arrived(FQ, out.at[2])
    arrived(MQ.at[pl.ds(0, 7)], out.at[3])
    arrived(MQ.at[pl.ds(0, 7)], out.at[4])
    arrived(WQ.at[pl.ds(0, 7), 0, :, 0], out.at[5])
    arrived(WQ.at[pl.ds(0, 7)], out.at[6])
    arrived(WQ, out.at[7])
    arrived(PB.at[:, :, 0], out.at[8])
    arrived(R1.at[:, pl.ds(0, 7)], out.at[9])
    arrived(R2.at[:, pl.ds(0, 7)], out.at[10])
    arrived(DQ.at[pl.ds(0, 7)], out.at[11])
    arrived(DQ, out.at[12])
    arrived(SX.at[pl.ds(0, 7)], out.at[13])
    arrived(TT.at[:, pl.ds(0, 7)], out.at[14])


def update_kernel(
    FQ, FK, WQ, WK, DQ, DK, total_ref, mom_ref,
    uq_out, nq_out, cq_out, f1q_out, f2q_out, uk_out, nk_out, ck_out, f1k_out, f2k_out,
    copies, own, mom, sems, small_sems,
):
    z, y, c = (lax.axis_index(a) for a in FS)
    F, W, Dn = (FQ, FK), (WQ, WK), (DQ, DK)
    outs = ((uq_out, nq_out, cq_out, f1q_out, f2q_out), (uk_out, nk_out, ck_out, f1k_out, f2k_out))
    flight = []
    mom[...] = mom_ref[...]
    for k in (0, 1):
        for m in (0, 1):
            copy = pltpu.make_async_copy(mom.at[k, m], outs[k][3 + m], small_sems.at[k, m])
            copy.start()
            flight.append(copy)
    for k in (0, 1):
        total = total_ref[k : k + 1, :]
        scale = 1.0 / jnp.maximum(jnp.sqrt(total * (1.0 / 262144.0)), scale_floor)
        high, low = two_pieces(Dn[k][...].reshape(256, 256))

        def update_of(rows):
            whole = jnp.dot(rows, high, preferred_element_type=f32) + jnp.dot(rows, low, preferred_element_type=f32)
            return -scale * whole

        for b in range(N):
            update = update_of(rows_of(F[k], k, b))
            new = rows_of(W[k], k, b) + learn_rate * update
            copies[k, b] = new.astype(bf16)
            copy = pltpu.make_async_copy(copies.at[k, b], outs[k][2].at[pl.ds(b * 256, 256), :], sems.at[k, b])
            copy.start()
            flight.append(copy)
        update = update_of(own_rows(F[k], k, z, y, c))
        own[k, 0] = update
        own[k, 1] = own_rows(W[k], k, z, y, c) + learn_rate * update
        for m in (0, 1):
            copy = pltpu.make_async_copy(own.at[k, m], outs[k][m], small_sems.at[k, 2 + m])
            copy.start()
            flight.append(copy)
    for copy in flight:
        copy.wait()


def body(*args):
    hbm = pl.BlockSpec(memory_space=pltpu.HBM)
    vmem = pl.BlockSpec(memory_space=pltpu.VMEM)
    shape = jax.ShapeDtypeStruct
    by_z, by_y = (8, 4, 2, 2, 16, 256), (4, 2, 8, 2, 16, 256)
    dma = pltpu.SemaphoreType.DMA
    room = pltpu.VMEM
    mid = pl.pallas_call(
        exchange_kernel,
        out_shape=(
            room(by_z, bf16), room(by_y, bf16), room(by_z, f32), room(by_y, f32),
            room((8, 2, 16, 256), f32), room((8, 2, 16, 256), f32), room((8, 256), f32), room((2, 2, 2, 256), f32),
        ),
        in_specs=[hbm] * 11,
        out_specs=(vmem,) * 8,
        scratch_shapes=[
            room((192, 2048), bf16), room((2, 192, 256), bf16), room((2, 16, 256), bf16),
            room((8, 2, 2, 256), f32), room((8, 2, 2, 256), f32), room((2, 2, 16, 256), f32),
            room((2, 8, 2, 16, 256), f32), room((2, 8, 16, 256), f32), room((2, 8, 16, 256), f32),
            room((2, 8, 16, 256), f32), room((2, 8, 16, 256), f32), room((8, 2, 128), f32), room((2, 8, 2, 128), f32),
            room((2, 2, 16, 256), f32), room((2, 2, 8, 2, 256), f32),
            dma((6,)), dma((15,)), dma((2, 4)), dma((2, 8, 2)), dma((2,)),
            dma((2,)), dma((2, 4)), dma((2, 4)), dma((2,)), dma((2,)), dma((2,)),
            dma((2,)), dma((2,)), dma((2,)), dma((2,)), dma((1,)), dma((2,)),
        ],
        compiler_params=pltpu.CompilerParams(collective_id=0, has_side_effects=True, vmem_limit_bytes=40 * 1024 * 1024),
    )(*(pltpu.with_memory_space_constraint(a, pltpu.HBM) for a in args))
    one = (
        shape((16, 256), f32), shape((16, 256), f32), shape((2048, 256), bf16), shape((2, 256), f32), shape((2, 256), f32),
    )
    return pl.pallas_call(
        update_kernel,
        out_shape=one + one,
        in_specs=[vmem] * 8,
        out_specs=(hbm,) * 10,
        scratch_shapes=[
            room((2, 8, 256, 256), bf16), room((2, 2, 16, 256), f32), room((2, 2, 2, 256), f32), dma((2, 8)), dma((2, 4)),
        ],
        compiler_params=pltpu.CompilerParams(vmem_limit_bytes=40 * 1024 * 1024),
    )(*mid)


def solution(mesh):
    split = Mesh(mesh.devices.reshape(8, 8, 2, mesh.shape["tp"]), ("z", "y", "c", "tp"))
    rows, tiles = P(FS, None), P(FS, "tp")
    one = (tiles, tiles, P(None, "tp"), tiles, tiles)
    return jax.shard_map(
        body,
        mesh=split,
        in_specs=(rows, tiles, tiles, rows, rows, tiles, tiles, tiles, tiles, tiles, tiles),
        out_specs=one + one,
        check_vma=False,
    )
```

```python
import jax
import jax.numpy as jnp
from jax import lax
from jax.experimental import pallas as pl
from jax.experimental.pallas import tpu as pltpu
from jax.sharding import Mesh
from jax.sharding import PartitionSpec as P

MESH = pl.DeviceIdType.MESH
FS = ("z", "y", "c")
N = 8
SUBS = 4
FAR_FIRST = (4, 3, 5, 2, 6, 1, 7)

beta_one = 0.9
beta_two = 0.99
denom_floor = 0.001
scale_floor = 0.5
learn_rate = 0.02

f32 = jnp.float32
bf16 = jnp.bfloat16


def two_pieces(v):
    high = v.astype(bf16)
    low = (v - high.astype(f32)).astype(bf16)
    return high, low


def ring(v, d):
    return lax.rem(v + (d + 2 * N), N)


class Part:
    def __init__(self, first, second, pos):
        self.first, self.second = first, second
        self.f, self.s, self.c = pos[first], pos[second], pos["c"]
        self.by_z = second == "z"

    def block(self, buf, f, s, c):
        return buf.at[s, f // 2, f % 2, c] if self.by_z else buf.at[f // 2, f % 2, s, c]

    def sub(self, buf, j, s, c):
        return buf.at[s, j, :, c] if self.by_z else buf.at[j, :, s, c]

    def half(self, buf, h, s, c):
        return buf.at[s, pl.ds(2 * h, 2), :, c] if self.by_z else buf.at[pl.ds(2 * h, 2), :, s, c]

    def strip(self, buf, s, c):
        return buf.at[s, :, :, c] if self.by_z else buf.at[:, :, s, c]

    def one_core(self, buf):
        return buf.at[:, :, :, 0]

    def peer(self, axis, d):
        return {axis: ring(self.f if axis == self.first else self.s, d)}


def rows_of(buf, k, b):
    return (buf[b] if k == 0 else buf[b // 2, b % 2]).reshape(256, 256)


def own_rows(buf, k, z, y, c):
    return buf[z, y // 2, y % 2, c] if k == 0 else buf[z // 2, z % 2, y, c]


def exchange_kernel(
    x_hbm, cq_hbm, ck_hbm, fq_hbm, fk_hbm, q1_hbm, q2_hbm, k1_hbm, k2_hbm, wq_hbm, wk_hbm,
    FQ, FK, WQ, WK, DQ, DK, total_ref, mom_ref,
    xv, cots, fown, MQ, MK, MF, PB, PR, SB, R1, R2, SX, TT, T, M8,
    loc, out, d1, r2, dd, w1, wr, wl, wd, ms, ps, b1, b2, c1, cd, xs, ts,
):
    pos = {a: lax.axis_index(a) for a in FS}
    x = lax.axis_index("tp")
    z, y, c = pos["z"], pos["y"], pos["c"]
    parts = (Part("y", "z", pos), Part("z", "y", pos))
    both = tuple(enumerate(parts))
    F, W, Dn, Mo = (FQ, FK), (WQ, WK), (DQ, DK), (MQ, MK)
    other = {"c": 1 - c}

    def send(src, dst, group, recv, to):
        pltpu.make_async_remote_copy(
            src_ref=src, dst_ref=dst, send_sem=out.at[group], recv_sem=recv, device_id=to, device_id_type=MESH
        ).start()

    def arrived(view, recv):
        pltpu.make_async_copy(view, view, recv).wait()

    def load(src, dst, sem):
        pltpu.make_async_copy(src, dst, loc.at[sem]).start()

    load(fq_hbm, fown.at[0], 0)
    load(fk_hbm, fown.at[1], 0)
    load(q1_hbm, MQ.at[z, 0], 1)
    load(q2_hbm, MQ.at[z, 1], 1)
    load(k1_hbm, MK.at[y, 0], 2)
    load(k2_hbm, MK.at[y, 1], 2)
    load(wq_hbm, parts[0].block(WQ, y, z, c), 3)
    load(wk_hbm, parts[1].block(WK, z, y, c), 3)
    load(cq_hbm, cots.at[0], 4)
    load(ck_hbm, cots.at[1], 4)
    load(x_hbm, xv, 5)

    barrier = pltpu.get_barrier_semaphore()
    greeted = [{"y": ring(y, d)} for d in range(1, N)] + [{"z": ring(z, d)} for d in range(1, N)] + [other]
    kin = []
    for d in range(1, 4):
        kin += [{"tp": lax.rem(x + d, 4)}, {"tp": lax.rem(x + d, 4), "c": 1 - c}]
    for to in greeted + kin:
        pl.semaphore_signal(barrier, inc=1, device_id=to, device_id_type=MESH)

    rank = lax.broadcasted_iota(jnp.int32, (256, 256), 0)
    slot = lax.broadcasted_iota(jnp.int32, (256, 256), 1)
    sf, sc, ss, si = slot >> 5, (slot >> 4) & 1, (slot >> 1) & 7, slot & 1
    places = (((ss * 8 + sf) * 2 + sc) * 2 + si, ((sf * 8 + ss) * 2 + sc) * 2 + si)
    arrived(fown, loc.at[0])
    for k, p in both:
        order = jnp.where(rank == places[k], 1.0, 0.0).astype(bf16)
        mine = jnp.dot(fown[k], order, preferred_element_type=f32).astype(bf16)
        p.block(F[k], p.f, p.s, c)[...] = mine
    arrived(MQ.at[0], loc.at[1])
    arrived(MK.at[0], loc.at[2])
    arrived(WQ.at[0, 0, :, 0], loc.at[3])
    pl.semaphore_wait(barrier, len(greeted) + len(kin))

    def direct(k, buf, group, recv_of):
        p = parts[k]
        mine = p.block(buf, p.f, p.s, c)
        for d in FAR_FIRST:
            send(mine, mine, group, recv_of(k, p, d), p.peer(p.first, d))

    def pair_sem(k, p, d):
        return d1.at[k, lax.rem(p.f // 2 - ring(p.f, d) // 2 + SUBS, SUBS)]

    for k in (0, 1):
        direct(k, F[k], 0, pair_sem)
    for k in (0, 1):
        direct(k, W[k], 5, lambda k, p, d: w1.at[k])

    def piece(p, n):
        return lax.rem(p.f // 2 + n, SUBS)

    for n in range(SUBS):
        for k, p in both:
            j = piece(p, n)
            mine = p.sub(F[k], j, p.s, c)
            arrived(p.block(F[k], 0, 0, 0) if n == 0 else mine, d1.at[k, n])
            for d in (2, -2, 1, -1):
                send(mine, mine, 1, r2.at[k, d + 3, n // 2], p.peer(p.second, d))
    for k, p in both:
        mine = p.strip(F[k], p.s, c)
        send(mine, mine, 2, dd.at[k], other)
    for h in (0, 1):
        for k, p in both:
            for way in (1, -1):
                src = ring(p.s, -2 * way)
                arrived(p.half(F[k], 0, src, c), r2.at[k, 2 * way + 3, h])
                for n in (2 * h, 2 * h + 1):
                    got = p.sub(F[k], piece(p, n), src, c)
                    if (h == 0) == (way == 1):
                        send(got, got, 1, r2.at[k, 7, h], p.peer(p.second, 2 * way))
                    send(got, got, 1, r2.at[k, 3 * way + 3, h], p.peer(p.second, way))
    for k, p in both:
        for d in (1, -1):
            for h in (0, 1):
                arrived(p.half(F[k], 0, p.s, c), r2.at[k, d + 3, h])
        for d in (1, -1, 2, -2):
            got = p.strip(F[k], ring(p.s, d), c)
            send(got, got, 2, dd.at[k], other)

    for k, p in both:
        for d in FAR_FIRST:
            mine = Mo[k].at[p.s]
            send(mine, mine, 3 + k, ms.at[k], p.peer(p.second, d))
    def weights_step(t):
        for k, p in both:
            right, left = p.peer(p.second, 1), p.peer(p.second, -1)
            if t == 0:
                arrived((WQ.at[pl.ds(0, 7), 0, 0, 0]), w1.at[k])
                mine = p.strip(W[k], p.s, c)
                send(mine, mine, 6, wr.at[k, 0], right)
                send(mine, mine, 6, wl.at[k, 0], left)
                send(mine, mine, 7, wd.at[k], other)
            elif t < 4:
                from_left = p.strip(W[k], ring(p.s, -t), c)
                arrived(from_left, wr.at[k, t - 1])
                from_right = p.strip(W[k], ring(p.s, t), c)
                arrived(from_right, wl.at[k, t - 1])
                if t < 3:
                    send(from_left, from_left, 6, wr.at[k, t], right)
                    send(from_right, from_right, 6, wl.at[k, t], left)
                else:
                    low, high = p.half(W[k], 0, ring(p.s, -3), c), p.half(W[k], 1, ring(p.s, 3), c)
                    send(low, low, 6, wr.at[k, 3], right)
                    send(high, high, 6, wl.at[k, 3], left)
                send(from_left, from_left, 7, wd.at[k], other)
                send(from_right, from_right, 7, wd.at[k], other)
            else:
                arrived(p.half(W[k], 0, ring(p.s, 4), c), wr.at[k, 3])
                arrived(p.half(W[k], 1, ring(p.s, 4), c), wl.at[k, 3])
                last = p.strip(W[k], ring(p.s, 4), c)
                send(last, last, 7, wd.at[k], other)

    weights_step(0)
    for k, p in both:
        for d in (3, -3, 4):
            for h in (0, 1):
                arrived(p.half(F[k], 0, p.s, c), r2.at[k, d + 3, h])
                for n in (2 * h, 2 * h + 1):
                    got = p.sub(F[k], piece(p, n), ring(p.s, -d), c)
                    send(got, got, 2, dd.at[k], other)

    arrived(cots, loc.at[4])
    arrived(xv, loc.at[5])
    for k, p in both:
        arrived(p.one_core(F[k]), dd.at[k])
        mixed = jnp.zeros((192, 256), f32)
        for b in range(N):
            mixed += jnp.dot(xv[:, b * 256 : (b + 1) * 256], rows_of(F[k], k, b), preferred_element_type=f32)
        high, low = two_pieces(mixed)
        product = jnp.dot(high.T, cots[k], preferred_element_type=f32)
        product += jnp.dot(low.T, cots[k], preferred_element_type=f32)
        PB[k] = product.reshape(N, 2, 16, 256)
        send(PB.at[k, :, 1 - c], PR.at[k], 8, ps.at[k], other)
    weights_step(1)

    for k, p in both:
        arrived(PR.at[k], ps.at[k])
        SB[k] = PB[k, :, c] + PR[k]
        for d in FAR_FIRST:
            to = ring(p.f, d)
            send(SB.at[k, to], R1.at[k, p.f], 9, b1.at[k], {p.first: to})
    weights_step(2)
    for k, p in both:
        arrived(R1.at[k, pl.ds(0, 7)], b1.at[k])
        acc = SB[k, p.f]
        for d in FAR_FIRST:
            acc += R1[k, ring(p.f, -d)]
        R2[k, p.s] = acc
        for d in FAR_FIRST:
            mine = R2.at[k, p.s]
            send(mine, mine, 10, b2.at[k], p.peer(p.second, d))
    for k, p in both:
        arrived(Mo[k].at[pl.ds(0, 7)], ms.at[k])
        for b in range(N):
            for m in (0, 1):
                MF[k, m, 2 * b : 2 * b + 2, :] = Mo[k][b, m]
    weights_step(3)

    sums = []
    for k, p in both:
        arrived(R2.at[k, pl.ds(0, 7)], b2.at[k])
        small = R2[k, 0]
        for b in range(1, N):
            small += R2[k, b]
        first_new = beta_one * MF[k, 0] + (1.0 - beta_one) * small
        second_new = beta_two * MF[k, 1] + (1.0 - beta_two) * small * small
        direction = first_new / (jnp.sqrt(second_new) + denom_floor)
        Dn[k][p.f, c] = direction
        for d in FAR_FIRST:
            mine = Dn[k].at[p.f, c]
            send(mine, mine, 11, c1.at[k], p.peer(p.first, d))
        sums.append(jnp.sum(direction * direction, axis=(0, 1), keepdims=True))
        T[k, 0] = first_new
        T[k, 1] = second_new

    row = lax.broadcasted_iota(jnp.int32, (2, 128), 0)
    SX[2 * x + c] = jnp.where(row == 0, sums[0], sums[1])
    for to in [other] + kin:
        mine = SX.at[2 * x + c]
        send(mine, mine, 13, xs.at[0], to)
    for k, p in both:
        for m in (0, 1):
            for b in range(N):
                M8[k, m, b] = T[k, m, 2 * b : 2 * b + 2, :]
            mom_ref[k, m] = M8[k, m, p.s]
    arrived(SX.at[pl.ds(0, 7)], xs.at[0])
    across = SX[0]
    for b in range(1, N):
        across += SX[b]
    for k, p in both:
        TT[k, p.f] = across
        for d in FAR_FIRST:
            mine = TT.at[k, p.f]
            send(mine, mine, 14, ts.at[k], p.peer(p.first, d))
    weights_step(4)
    for k, p in both:
        arrived(DQ.at[pl.ds(0, 7), 0], c1.at[k])
        mine = Dn[k].at[:, c]
        send(mine, mine, 12, cd.at[k], other)
    totals = []
    for k in (0, 1):
        arrived(TT.at[k, pl.ds(0, 7)], ts.at[k])
        total = TT[k, 0]
        for b in range(1, N):
            total += TT[k, b]
        totals.append(total[k : k + 1, 0:1])
    lane = lax.broadcasted_iota(jnp.int32, (8, 256), 0)
    total_ref[...] = jnp.where(lane == 0, totals[0], totals[1])
    for k, p in both:
        arrived(DQ.at[:, 0], cd.at[k])
        arrived(p.one_core(W[k]), wd.at[k])

    arrived(FQ.at[pl.ds(0, 7), 0, :, 0], out.at[0])
    arrived(FQ.at[pl.ds(0, 7)], out.at[1])
    arrived(FQ, out.at[2])
    arrived(MQ.at[pl.ds(0, 7)], out.at[3])
    arrived(MQ.at[pl.ds(0, 7)], out.at[4])
    arrived(WQ.at[pl.ds(0, 7), 0, :, 0], out.at[5])
    arrived(WQ.at[pl.ds(0, 7)], out.at[6])
    arrived(WQ, out.at[7])
    arrived(PB.at[:, :, 0], out.at[8])
    arrived(R1.at[:, pl.ds(0, 7)], out.at[9])
    arrived(R2.at[:, pl.ds(0, 7)], out.at[10])
    arrived(DQ.at[pl.ds(0, 7)], out.at[11])
    arrived(DQ, out.at[12])
    arrived(SX.at[pl.ds(0, 7)], out.at[13])
    arrived(TT.at[:, pl.ds(0, 7)], out.at[14])


def update_kernel(
    FQ, FK, WQ, WK, DQ, DK, total_ref, mom_ref,
    uq_out, nq_out, cq_out, f1q_out, f2q_out, uk_out, nk_out, ck_out, f1k_out, f2k_out,
    copies, own, mom, sems, small_sems,
):
    z, y, c = (lax.axis_index(a) for a in FS)
    F, W, Dn = (FQ, FK), (WQ, WK), (DQ, DK)
    outs = ((uq_out, nq_out, cq_out, f1q_out, f2q_out), (uk_out, nk_out, ck_out, f1k_out, f2k_out))
    flight = []
    mom[...] = mom_ref[...]
    for k in (0, 1):
        for m in (0, 1):
            copy = pltpu.make_async_copy(mom.at[k, m], outs[k][3 + m], small_sems.at[k, m])
            copy.start()
            flight.append(copy)
    for k in (0, 1):
        total = total_ref[k : k + 1, :]
        scale = 1.0 / jnp.maximum(jnp.sqrt(total * (1.0 / 262144.0)), scale_floor)
        high, low = two_pieces(Dn[k][...].reshape(256, 256))

        def update_of(rows):
            whole = jnp.dot(rows, high, preferred_element_type=f32) + jnp.dot(rows, low, preferred_element_type=f32)
            return -scale * whole

        for b in range(N):
            update = update_of(rows_of(F[k], k, b))
            new = rows_of(W[k], k, b) + learn_rate * update
            copies[k, b] = new.astype(bf16)
            copy = pltpu.make_async_copy(copies.at[k, b], outs[k][2].at[pl.ds(b * 256, 256), :], sems.at[k, b])
            copy.start()
            flight.append(copy)
        update = update_of(own_rows(F[k], k, z, y, c))
        own[k, 0] = update
        own[k, 1] = own_rows(W[k], k, z, y, c) + learn_rate * update
        for m in (0, 1):
            copy = pltpu.make_async_copy(own.at[k, m], outs[k][m], small_sems.at[k, 2 + m])
            copy.start()
            flight.append(copy)
    for copy in flight:
        copy.wait()


def body(*args):
    hbm = pl.BlockSpec(memory_space=pltpu.HBM)
    vmem = pl.BlockSpec(memory_space=pltpu.VMEM)
    shape = jax.ShapeDtypeStruct
    by_z, by_y = (8, 4, 2, 2, 16, 256), (4, 2, 8, 2, 16, 256)
    dma = pltpu.SemaphoreType.DMA
    room = pltpu.VMEM
    mid = pl.pallas_call(
        exchange_kernel,
        out_shape=(
            room(by_z, bf16), room(by_y, bf16), room(by_z, f32), room(by_y, f32),
            room((8, 2, 16, 256), f32), room((8, 2, 16, 256), f32), room((8, 256), f32), room((2, 2, 2, 256), f32),
        ),
        in_specs=[hbm] * 11,
        out_specs=(vmem,) * 8,
        scratch_shapes=[
            room((192, 2048), bf16), room((2, 192, 256), bf16), room((2, 16, 256), bf16),
            room((8, 2, 2, 256), f32), room((8, 2, 2, 256), f32), room((2, 2, 16, 256), f32),
            room((2, 8, 2, 16, 256), f32), room((2, 8, 16, 256), f32), room((2, 8, 16, 256), f32),
            room((2, 8, 16, 256), f32), room((2, 8, 16, 256), f32), room((8, 2, 128), f32), room((2, 8, 2, 128), f32),
            room((2, 2, 16, 256), f32), room((2, 2, 8, 2, 256), f32),
            dma((6,)), dma((15,)), dma((2, 4)), dma((2, 8, 2)), dma((2,)),
            dma((2,)), dma((2, 4)), dma((2, 4)), dma((2,)), dma((2,)), dma((2,)),
            dma((2,)), dma((2,)), dma((2,)), dma((2,)), dma((1,)), dma((2,)),
        ],
        compiler_params=pltpu.CompilerParams(collective_id=0, has_side_effects=True, vmem_limit_bytes=40 * 1024 * 1024),
    )(*(pltpu.with_memory_space_constraint(a, pltpu.HBM) for a in args))
    one = (
        shape((16, 256), f32), shape((16, 256), f32), shape((2048, 256), bf16), shape((2, 256), f32), shape((2, 256), f32),
    )
    return pl.pallas_call(
        update_kernel,
        out_shape=one + one,
        in_specs=[vmem] * 8,
        out_specs=(hbm,) * 10,
        scratch_shapes=[
            room((2, 8, 256, 256), bf16), room((2, 2, 16, 256), f32), room((2, 2, 2, 256), f32), dma((2, 8)), dma((2, 4)),
        ],
        compiler_params=pltpu.CompilerParams(vmem_limit_bytes=40 * 1024 * 1024),
    )(*mid)


def solution(mesh):
    split = Mesh(mesh.devices.reshape(8, 8, 2, mesh.shape["tp"]), ("z", "y", "c", "tp"))
    rows, tiles = P(FS, None), P(FS, "tp")
    one = (tiles, tiles, P(None, "tp"), tiles, tiles)
    return jax.shard_map(
        body,
        mesh=split,
        in_specs=(rows, tiles, tiles, rows, rows, tiles, tiles, tiles, tiles, tiles, tiles),
        out_specs=one + one,
        check_vma=False,
    )
```

```python
import jax
import jax.numpy as jnp
from jax import lax
from jax.experimental import pallas as pl
from jax.experimental.pallas import tpu as pltpu
from jax.sharding import Mesh
from jax.sharding import PartitionSpec as P

MESH = pl.DeviceIdType.MESH
FS = ("z", "y", "c")
N = 8
FAR_FIRST = (4, 3, 5, 2, 6, 1, 7)
NEAR_FIRST = (1, 7, 2, 6, 3, 5, 4)

beta_one = 0.9
beta_two = 0.99
denom_floor = 0.001
scale_floor = 0.5
learn_rate = 0.02

f32 = jnp.float32
bf16 = jnp.bfloat16


def two_pieces(v):
    high = v.astype(bf16)
    low = (v - high.astype(f32)).astype(bf16)
    return high, low


def ring(v, d):
    return lax.rem(v + (d + 2 * N), N)


class Part:
    def __init__(self, first, second, pos):
        self.first, self.second = first, second
        self.f, self.s, self.c = pos[first], pos[second], pos["c"]
        self.by_z = second == "z"

    def block(self, buf, f, s, c):
        return buf.at[s, f // 2, f % 2, c] if self.by_z else buf.at[f // 2, f % 2, s, c]

    def half(self, buf, h, s, c):
        return buf.at[s, pl.ds(2 * h, 2), :, c] if self.by_z else buf.at[pl.ds(2 * h, 2), :, s, c]

    def strip(self, buf, s, c):
        return buf.at[s, :, :, c] if self.by_z else buf.at[:, :, s, c]

    def one_core(self, buf):
        return buf.at[:, :, :, 0]

    def peer(self, axis, d):
        return {axis: ring(self.f if axis == self.first else self.s, d)}


def assemble(FULL, plane, b):
    pair = jnp.stack([FULL[plane, 0, b], FULL[plane, 1, :, b]], axis=1)
    return pair.reshape(256, 128)


def rows_of(buf, k, b):
    return (buf[b] if k == 0 else buf[b // 2, b % 2]).reshape(256, 256)


def own_rows(buf, k, z, y, c):
    return buf[z, y // 2, y % 2, c] if k == 0 else buf[z // 2, z % 2, y, c]


def exchange_kernel(
    x_hbm, cq_hbm, ck_hbm, fq_hbm, fk_hbm, q1_hbm, q2_hbm, k1_hbm, k2_hbm, wq_hbm, wk_hbm,
    FULL, WQ, WK, DD, total_ref, mom_ref,
    xv, cots, CA, fown, MOM, MF, PB, PR, SB, R1, S1, R2, TS, T, M8,
    loc, out, inn, r2, w1, wr, wl, wd,
):
    pos = {a: lax.axis_index(a) for a in FS}
    x = lax.axis_index("tp")
    z, y, c = pos["z"], pos["y"], pos["c"]
    both = tuple(enumerate((Part("y", "z", pos), Part("z", "y", pos))))
    W = (WQ, WK)
    other = {"c": 1 - c}
    first_is_y = c == 0
    f, s = jnp.where(first_is_y, y, z), jnp.where(first_is_y, z, y)
    proj, side = x // 2, x % 2
    D1, DDUP, MS, CS, PS, B1, B2, C1, CD, TSUM, FX, FD = range(12)

    def on_first(d):
        return {"y": jnp.where(first_is_y, ring(y, d), y), "z": jnp.where(first_is_y, z, ring(z, d))}

    def on_second(d):
        return {"y": jnp.where(first_is_y, y, ring(y, d)), "z": jnp.where(first_is_y, ring(z, d), z)}

    def plane(d):
        return lax.rem(x + d, 4)

    def send(src, dst, group, recv, to):
        pltpu.make_async_remote_copy(
            src_ref=src, dst_ref=dst, send_sem=out.at[group], recv_sem=recv, device_id=to, device_id_type=MESH
        ).start()

    def same(ref, group, recv, to):
        send(ref, ref, group, recv, to)

    def arrived(view, recv):
        pltpu.make_async_copy(view, view, recv).wait()

    def load(src, dst, sem):
        pltpu.make_async_copy(src, dst, loc.at[sem]).start()

    load(fq_hbm, fown.at[0], 0)
    load(fk_hbm, fown.at[1], 0)
    load(cq_hbm, cots.at[0], 4)
    load(ck_hbm, cots.at[1], 4)
    load(wq_hbm, both[0][1].block(WQ, y, z, c), 3)
    load(wk_hbm, both[1][1].block(WK, z, y, c), 3)
    load(q1_hbm, MOM.at[s, 0, 0], 1)
    load(q2_hbm, MOM.at[s, 0, 1], 1)
    load(k1_hbm, MOM.at[s, 1, 0], 1)
    load(k2_hbm, MOM.at[s, 1, 1], 1)

    @pl.when(proj == 0)
    def _():
        load(cq_hbm, CA.at[x], 2)

    @pl.when(proj == 1)
    def _():
        load(ck_hbm, CA.at[x], 2)

    load(x_hbm, xv, 5)

    barrier = pltpu.get_barrier_semaphore()
    greeted = [{"y": ring(y, d)} for d in range(1, N)] + [{"z": ring(z, d)} for d in range(1, N)] + [other]
    for d in range(1, 4):
        greeted += [{"tp": plane(d)}, {"tp": plane(d), "c": 1 - c}]
    for to in greeted:
        pl.semaphore_signal(barrier, inc=1, device_id=to, device_id_type=MESH)

    rank = lax.broadcasted_iota(jnp.int32, (256, 128), 0)
    lane = lax.broadcasted_iota(jnp.int32, (256, 128), 1)
    lc, lf, ls, li = lane >> 6, (lane >> 3) & 7, ((lane >> 1) & 3) + 4 * side, lane & 1
    lz, ly = jnp.where(lc == 0, ls, lf), jnp.where(lc == 0, lf, ls)
    order = jnp.where(rank == ((lz * 8 + ly) * 2 + lc) * 2 + li, 1.0, 0.0).astype(bf16)
    arrived(fown, loc.at[0])
    FULL[x, c, s, f] = jnp.dot(fown[proj], order, preferred_element_type=f32).astype(bf16)
    arrived(cots, loc.at[4])
    arrived(WQ.at[0, 0, :, 0], loc.at[3])
    arrived(MOM.at[0], loc.at[1])
    pl.semaphore_wait(barrier, len(greeted))

    for d in FAR_FIRST:
        same(FULL.at[x, c, s, f], 0, inn.at[D1], on_first(d))
    for d in (2, 1, 3):
        send(cots.at[plane(d) // 2], CA.at[x], 4, inn.at[CS], {"tp": plane(d)})
    for k, p in both:
        mine = p.block(W[k], p.f, p.s, c)
        for d in FAR_FIRST:
            same(mine, 5, w1.at[k], p.peer(p.first, d))
    for d in FAR_FIRST:
        same(MOM.at[s], 3, inn.at[MS], on_second(d))

    arrived(FULL.at[0, 0, 0, pl.ds(0, 7)], inn.at[D1])
    for d in FAR_FIRST:
        same(FULL.at[x, c, s], 1, r2.at[d], on_second(d))
    same(FULL.at[x, c, s], 2, inn.at[DDUP], other)

    def weights_step(t):
        for k, p in both:
            right, left = p.peer(p.second, 1), p.peer(p.second, -1)
            if t == 0:
                arrived(WQ.at[pl.ds(0, 7), 0, 0, 0], w1.at[k])
                mine = p.strip(W[k], p.s, c)
                same(mine, 6, wr.at[k, 0], right)
                same(mine, 6, wl.at[k, 0], left)
                same(mine, 7, wd.at[k], other)
            elif t < 4:
                from_left = p.strip(W[k], ring(p.s, -t), c)
                arrived(from_left, wr.at[k, t - 1])
                from_right = p.strip(W[k], ring(p.s, t), c)
                arrived(from_right, wl.at[k, t - 1])
                if t < 3:
                    same(from_left, 6, wr.at[k, t], right)
                    same(from_right, 6, wl.at[k, t], left)
                else:
                    same(p.half(W[k], 0, ring(p.s, -3), c), 6, wr.at[k, 3], right)
                    same(p.half(W[k], 1, ring(p.s, 3), c), 6, wl.at[k, 3], left)
                same(from_left, 7, wd.at[k], other)
                same(from_right, 7, wd.at[k], other)
            else:
                arrived(p.half(W[k], 0, ring(p.s, 4), c), wr.at[k, 3])
                arrived(p.half(W[k], 1, ring(p.s, 4), c), wl.at[k, 3])
                same(p.strip(W[k], ring(p.s, 4), c), 7, wd.at[k], other)

    weights_step(0)
    for d in NEAR_FIRST:
        arrived(FULL.at[0, 0, 0], r2.at[d])
        same(FULL.at[x, c, ring(s, -d)], 2, inn.at[DDUP], other)
    for d in (2, 1, 3):
        same(FULL.at[x, c], 14, inn.at[FX], {"tp": plane(d)})

    arrived(xv, loc.at[5])
    arrived(CA.at[0], loc.at[2])
    arrived(CA.at[pl.ds(0, 3)], inn.at[CS])
    arrived(FULL.at[0, 0], inn.at[DDUP])
    mixed = jnp.zeros((192, 128), f32)
    for b in range(N):
        mixed += jnp.dot(xv[:, b * 256 : (b + 1) * 256], assemble(FULL, x, b), preferred_element_type=f32)
    high, low = two_pieces(mixed)
    pieces = jnp.concatenate([high.T, low.T], axis=0)
    for b in range(4):
        product = jnp.dot(pieces, CA[b], preferred_element_type=f32)
        PB[:, :, b] = (product[:128] + product[128:]).reshape(2, N, 8, 256)
        send(PB.at[1 - c, :, b], PR.at[:, b], 8, inn.at[PS], other)
    weights_step(1)

    arrived(PR, inn.at[PS])
    SB[...] = PB[c] + PR[...]
    for d in FAR_FIRST:
        send(SB.at[ring(f, d)], R1.at[f], 9, inn.at[B1], on_first(d))
    weights_step(2)
    arrived(R1.at[pl.ds(0, 7)], inn.at[B1])
    acc = SB[f]
    for d in FAR_FIRST:
        acc += R1[ring(f, -d)]
    S1[...] = acc

    for d in FAR_FIRST + (0,):
        for e in (2, 1, 3, 0):
            if d or e:
                send(S1.at[plane(e)], R2.at[x * N + s], 10, inn.at[B2], {**on_second(d), "tp": plane(e)})
    R2[x * N + s] = S1[x]
    weights_step(3)
    arrived(FULL.at[pl.ds(0, 3), 0], inn.at[FX])
    for d in (1, 2, 3):
        same(FULL.at[plane(d), c], 15, inn.at[FD], other)
    arrived(MOM.at[pl.ds(0, 7)], inn.at[MS])
    for k in (0, 1):
        for m in (0, 1):
            for b in range(N):
                MF[k, m, b // 4, 2 * (b % 4) : 2 * (b % 4) + 2, :] = MOM[b, k, m]

    arrived(R2.at[pl.ds(0, 31)], inn.at[B2])
    sums = []
    for k in (0, 1):
        squares = 0.0
        for h in (0, 1):
            at = (2 * k + h) * N
            small = R2[at]
            for b in range(1, N):
                small += R2[at + b]
            first_new = beta_one * MF[k, 0, h] + (1.0 - beta_one) * small
            second_new = beta_two * MF[k, 1, h] + (1.0 - beta_two) * small * small
            direction = first_new / (jnp.sqrt(second_new) + denom_floor)
            DD[c, f, k, h] = direction
            squares += direction * direction
            T[k, 0, h] = first_new
            T[k, 1, h] = second_new
        sums.append(jnp.sum(squares, axis=(0, 1), keepdims=True))
    for d in FAR_FIRST:
        same(DD.at[c, f], 11, inn.at[C1], on_first(d))

    row = lax.broadcasted_iota(jnp.int32, (2, 128), 0)
    mine = (c * N + f) * 4 + x
    TS[mine] = jnp.where(row == 0, sums[0], sums[1])
    for d in FAR_FIRST + (0,):
        for e in (2, 1, 3, 0):
            for core in (c, 1 - c):
                if d or e or core is not c:
                    same(TS.at[mine], 13, inn.at[TSUM], {**on_first(d), "tp": plane(e), "c": core})
    weights_step(4)
    for k in (0, 1):
        for m in (0, 1):
            for b in range(N):
                M8[k, m, b] = T[k, m, b // 4, 2 * (b % 4) : 2 * (b % 4) + 2, :]
            mom_ref[k, m] = M8[k, m, s]
    arrived(DD.at[0, pl.ds(0, 7)], inn.at[C1])
    same(DD.at[c], 12, inn.at[CD], other)
    arrived(TS.at[pl.ds(0, 63)], inn.at[TSUM])
    total = TS[0]
    for b in range(1, 64):
        total += TS[b]
    line = lax.broadcasted_iota(jnp.int32, (8, 256), 0)
    total_ref[...] = jnp.where(line == 0, total[0:1, 0:1], total[1:2, 0:1])
    arrived(DD.at[0], inn.at[CD])
    arrived(FULL.at[pl.ds(0, 3), 0], inn.at[FD])
    for k, p in both:
        arrived(p.one_core(W[k]), wd.at[k])

    for group, view in enumerate((
        FULL.at[0, 0, 0, pl.ds(0, 7)], FULL.at[0, 0, pl.ds(0, 7)], FULL.at[0, 0], MOM.at[pl.ds(0, 7)],
        CA.at[pl.ds(0, 3)], WQ.at[pl.ds(0, 7), 0, :, 0], WQ.at[pl.ds(0, 7)], WQ, PB.at[0], R1.at[pl.ds(0, 7)],
        R2.at[pl.ds(0, 31)], DD.at[0, pl.ds(0, 7)], DD.at[0], TS.at[pl.ds(0, 63)],
        FULL.at[pl.ds(0, 3), 0], FULL.at[pl.ds(0, 3), 0],
    )):
        arrived(view, out.at[group])


def update_kernel(
    FULL, WQ, WK, DD, total_ref, mom_ref,
    uq_out, nq_out, cq_out, f1q_out, f2q_out, uk_out, nk_out, ck_out, f1k_out, f2k_out,
    copies, own, mom, sems, small_sems,
):
    z, y, c = (lax.axis_index(a) for a in FS)
    f, s = jnp.where(c == 0, y, z), jnp.where(c == 0, z, y)
    W = (WQ, WK)
    outs = ((uq_out, nq_out, cq_out, f1q_out, f2q_out), (uk_out, nk_out, ck_out, f1k_out, f2k_out))
    flight = []
    mom[...] = mom_ref[...]
    for k in (0, 1):
        for m in (0, 1):
            copy = pltpu.make_async_copy(mom.at[k, m], outs[k][3 + m], small_sems.at[k, m])
            copy.start()
            flight.append(copy)
    for k in (0, 1):
        total = total_ref[k : k + 1, :]
        scale = 1.0 / jnp.maximum(jnp.sqrt(total * (1.0 / 262144.0)), scale_floor)
        full = jnp.concatenate([DD[:, :, k, h].reshape(128, 256) for h in (0, 1)], axis=0)
        high, low = two_pieces(full)

        def update_of(rows):
            whole = jnp.dot(rows, high, preferred_element_type=f32) + jnp.dot(rows, low, preferred_element_type=f32)
            return -scale * whole

        for b in range(N):
            rows = jnp.concatenate([assemble(FULL, 2 * k, b), assemble(FULL, 2 * k + 1, b)], axis=1)
            new = rows_of(W[k], k, b) + learn_rate * update_of(rows)
            copies[k, b] = new.astype(bf16)
            copy = pltpu.make_async_copy(copies.at[k, b], outs[k][2].at[pl.ds(b * 256, 256), :], sems.at[k, b])
            copy.start()
            flight.append(copy)
        update = update_of(jnp.concatenate([FULL[2 * k, c, s, f], FULL[2 * k + 1, c, s, f]], axis=1))
        own[k, 0] = update
        own[k, 1] = own_rows(W[k], k, z, y, c) + learn_rate * update
        for m in (0, 1):
            copy = pltpu.make_async_copy(own.at[k, m], outs[k][m], small_sems.at[k, 2 + m])
            copy.start()
            flight.append(copy)
    for copy in flight:
        copy.wait()


def body(*args):
    hbm = pl.BlockSpec(memory_space=pltpu.HBM)
    vmem = pl.BlockSpec(memory_space=pltpu.VMEM)
    shape = jax.ShapeDtypeStruct
    by_z, by_y = (8, 4, 2, 2, 16, 256), (4, 2, 8, 2, 16, 256)
    dma = pltpu.SemaphoreType.DMA
    room = pltpu.VMEM
    mid = pl.pallas_call(
        exchange_kernel,
        out_shape=(
            room((4, 2, 8, 8, 16, 128), bf16), room(by_z, f32), room(by_y, f32),
            room((2, 8, 2, 2, 8, 256), f32), room((8, 256), f32), room((2, 2, 2, 256), f32),
        ),
        in_specs=[hbm] * 11,
        out_specs=(vmem,) * 6,
        scratch_shapes=[
            room((192, 2048), bf16), room((2, 192, 256), bf16), room((4, 192, 256), bf16), room((2, 16, 256), bf16),
            room((8, 2, 2, 2, 256), f32), room((2, 2, 2, 8, 256), f32),
            room((2, 8, 4, 8, 256), f32), room((8, 4, 8, 256), f32), room((8, 4, 8, 256), f32), room((8, 4, 8, 256), f32),
            room((4, 8, 256), f32), room((32, 8, 256), f32), room((64, 2, 128), f32),
            room((2, 2, 2, 8, 256), f32), room((2, 2, 8, 2, 256), f32),
            dma((6,)), dma((16,)), dma((12,)), dma((8,)), dma((2,)), dma((2, 4)), dma((2, 4)), dma((2,)),
        ],
        compiler_params=pltpu.CompilerParams(collective_id=0, has_side_effects=True, vmem_limit_bytes=40 * 1024 * 1024),
    )(*(pltpu.with_memory_space_constraint(a, pltpu.HBM) for a in args))
    one = (
        shape((16, 256), f32), shape((16, 256), f32), shape((2048, 256), bf16), shape((2, 256), f32), shape((2, 256), f32),
    )
    return pl.pallas_call(
        update_kernel,
        out_shape=one + one,
        in_specs=[vmem] * 6,
        out_specs=(hbm,) * 10,
        scratch_shapes=[
            room((2, 8, 256, 256), bf16), room((2, 2, 16, 256), f32), room((2, 2, 2, 256), f32), dma((2, 8)), dma((2, 4)),
        ],
        compiler_params=pltpu.CompilerParams(vmem_limit_bytes=40 * 1024 * 1024),
    )(*mid)


def solution(mesh):
    split = Mesh(mesh.devices.reshape(8, 8, 2, mesh.shape["tp"]), ("z", "y", "c", "tp"))
    rows, tiles = P(FS, None), P(FS, "tp")
    one = (tiles, tiles, P(None, "tp"), tiles, tiles)
    return jax.shard_map(
        body,
        mesh=split,
        in_specs=(rows, tiles, tiles, rows, rows, tiles, tiles, tiles, tiles, tiles, tiles),
        out_specs=one + one,
        check_vma=False,
    )
```

```python
import jax
import jax.numpy as jnp
from jax import lax
from jax.experimental import pallas as pl
from jax.experimental.pallas import tpu as pltpu
from jax.sharding import Mesh
from jax.sharding import PartitionSpec as P

MESH = pl.DeviceIdType.MESH
FS = ("z", "y", "c")
N = 8
FAR_FIRST = (4, 3, 5, 2, 6, 1, 7)

beta_one = 0.9
beta_two = 0.99
denom_floor = 0.001
scale_floor = 0.5
learn_rate = 0.02

f32 = jnp.float32
bf16 = jnp.bfloat16


def two_pieces(v):
    high = v.astype(bf16)
    low = (v - high.astype(f32)).astype(bf16)
    return high, low


def ring(v, d):
    return lax.rem(v + (d + 2 * N), N)


class Part:
    def __init__(self, first, second, pos):
        self.first, self.second = first, second
        self.f, self.s, self.c = pos[first], pos[second], pos["c"]
        self.by_z = second == "z"

    def block(self, buf, f, s, c):
        return buf.at[s, f // 2, f % 2, c] if self.by_z else buf.at[f // 2, f % 2, s, c]

    def half(self, buf, h, s, c):
        return buf.at[s, pl.ds(2 * h, 2), :, c] if self.by_z else buf.at[pl.ds(2 * h, 2), :, s, c]

    def strip(self, buf, s, c):
        return buf.at[s, :, :, c] if self.by_z else buf.at[:, :, s, c]

    def one_core(self, buf):
        return buf.at[:, :, :, 0]

    def peer(self, axis, d):
        return {axis: ring(self.f if axis == self.first else self.s, d)}


def assemble(FULL, plane, b):
    pair = jnp.stack([FULL[plane, 0, b], FULL[plane, 1, :, b]], axis=1)
    return pair.reshape(256, 128)


def rows_of(buf, k, b):
    return (buf[b] if k == 0 else buf[b // 2, b % 2]).reshape(256, 256)


def own_rows(buf, k, z, y, c):
    return buf[z, y // 2, y % 2, c] if k == 0 else buf[z // 2, z % 2, y, c]


def exchange_kernel(
    x_hbm, cq_hbm, ck_hbm, fq_hbm, fk_hbm, q1_hbm, q2_hbm, k1_hbm, k2_hbm, wq_hbm, wk_hbm,
    FULL, WQ, WK, DD, total_ref, mom_ref,
    xv, cots, CA, fown, MOM, MF, PB, PR, SB, R1, S1, R2, TS, T, M8,
    loc, out, inn, fx, r2, c1, w1, wr, wl, wd,
):
    pos = {a: lax.axis_index(a) for a in FS}
    x = lax.axis_index("tp")
    z, y, c = pos["z"], pos["y"], pos["c"]
    both = tuple(enumerate((Part("y", "z", pos), Part("z", "y", pos))))
    W = (WQ, WK)
    other = {"c": 1 - c}
    first_is_y = c == 0
    f, s = jnp.where(first_is_y, y, z), jnp.where(first_is_y, z, y)
    proj, side = x // 2, x % 2
    D1, DDUP, MS, CS, PS, B1, B2, CD, TSUM, FD = range(10)

    def on_first(d):
        return {"y": jnp.where(first_is_y, ring(y, d), y), "z": jnp.where(first_is_y, z, ring(z, d))}

    def on_second(d):
        return {"y": jnp.where(first_is_y, y, ring(y, d)), "z": jnp.where(first_is_y, ring(z, d), z)}

    def plane(d):
        return lax.rem(x + d, 4)

    def send(src, dst, group, recv, to):
        pltpu.make_async_remote_copy(
            src_ref=src, dst_ref=dst, send_sem=out.at[group], recv_sem=recv, device_id=to, device_id_type=MESH
        ).start()

    def same(ref, group, recv, to):
        send(ref, ref, group, recv, to)

    def arrived(view, recv):
        pltpu.make_async_copy(view, view, recv).wait()

    def load(src, dst, sem):
        pltpu.make_async_copy(src, dst, loc.at[sem]).start()

    load(fq_hbm, fown.at[0], 0)
    load(fk_hbm, fown.at[1], 0)
    load(cq_hbm, cots.at[0], 4)
    load(ck_hbm, cots.at[1], 4)
    load(wq_hbm, both[0][1].block(WQ, y, z, c), 3)
    load(wk_hbm, both[1][1].block(WK, z, y, c), 3)
    load(q1_hbm, MOM.at[s, 0, 0], 1)
    load(q2_hbm, MOM.at[s, 0, 1], 1)
    load(k1_hbm, MOM.at[s, 1, 0], 1)
    load(k2_hbm, MOM.at[s, 1, 1], 1)

    @pl.when(proj == 0)
    def _():
        load(cq_hbm, CA.at[x], 2)

    @pl.when(proj == 1)
    def _():
        load(ck_hbm, CA.at[x], 2)

    load(x_hbm, xv, 5)

    barrier = pltpu.get_barrier_semaphore()
    greeted = [{"y": ring(y, d)} for d in range(1, N)] + [{"z": ring(z, d)} for d in range(1, N)] + [other]
    for d in range(1, 4):
        greeted += [{"tp": plane(d)}, {"tp": plane(d), "c": 1 - c}]
    for to in greeted:
        pl.semaphore_signal(barrier, inc=1, device_id=to, device_id_type=MESH)

    rank = lax.broadcasted_iota(jnp.int32, (256, 128), 0)
    lane = lax.broadcasted_iota(jnp.int32, (256, 128), 1)
    lc, lf, ls, li = lane >> 6, (lane >> 3) & 7, ((lane >> 1) & 3) + 4 * side, lane & 1
    lz, ly = jnp.where(lc == 0, ls, lf), jnp.where(lc == 0, lf, ls)
    order = jnp.where(rank == ((lz * 8 + ly) * 2 + lc) * 2 + li, 1.0, 0.0).astype(bf16)
    arrived(fown, loc.at[0])
    FULL[x, c, s, f] = jnp.dot(fown[proj], order, preferred_element_type=f32).astype(bf16)
    arrived(cots, loc.at[4])
    arrived(WQ.at[0, 0, :, 0], loc.at[3])
    arrived(MOM.at[0], loc.at[1])
    pl.semaphore_wait(barrier, len(greeted))

    for d in FAR_FIRST:
        same(FULL.at[x, c, s, f], 0, inn.at[D1], on_first(d))
    for d in (2, 1, 3):
        send(cots.at[plane(d) // 2], CA.at[x], 4, inn.at[CS], {"tp": plane(d)})
    for k, p in both:
        mine = p.block(W[k], p.f, p.s, c)
        for d in FAR_FIRST:
            same(mine, 5, w1.at[k], p.peer(p.first, d))
    for d in FAR_FIRST:
        same(MOM.at[s], 3, inn.at[MS], on_second(d))

    arrived(FULL.at[0, 0, 0, pl.ds(0, 7)], inn.at[D1])
    for d in FAR_FIRST:
        same(FULL.at[x, c, s], 1, r2.at[d], on_second(d))
    same(FULL.at[x, c, s], 2, inn.at[DDUP], other)

    def weights_step(t):
        for k, p in both:
            right, left = p.peer(p.second, 1), p.peer(p.second, -1)
            if t == 0:
                arrived(WQ.at[pl.ds(0, 7), 0, 0, 0], w1.at[k])
                mine = p.strip(W[k], p.s, c)
                same(mine, 6, wr.at[k, 0], right)
                same(mine, 6, wl.at[k, 0], left)
                same(mine, 7, wd.at[k], other)
            elif t < 4:
                from_left = p.strip(W[k], ring(p.s, -t), c)
                arrived(from_left, wr.at[k, t - 1])
                from_right = p.strip(W[k], ring(p.s, t), c)
                arrived(from_right, wl.at[k, t - 1])
                if t < 3:
                    same(from_left, 6, wr.at[k, t], right)
                    same(from_right, 6, wl.at[k, t], left)
                else:
                    same(p.half(W[k], 0, ring(p.s, -3), c), 6, wr.at[k, 3], right)
                    same(p.half(W[k], 1, ring(p.s, 3), c), 6, wl.at[k, 3], left)
                same(from_left, 7, wd.at[k], other)
                same(from_right, 7, wd.at[k], other)
            else:
                arrived(p.half(W[k], 0, ring(p.s, 4), c), wr.at[k, 3])
                arrived(p.half(W[k], 1, ring(p.s, 4), c), wl.at[k, 3])
                same(p.strip(W[k], ring(p.s, 4), c), 7, wd.at[k], other)

    weights_step(0)
    for d in FAR_FIRST:
        arrived(FULL.at[0, 0, 0], r2.at[d])
        same(FULL.at[x, c, ring(s, -d)], 2, inn.at[DDUP], other)
    for d in (1, 3):
        same(FULL.at[x, c], 14, fx.at[d], {"tp": plane(d)})

    arrived(xv, loc.at[5])
    arrived(CA.at[0], loc.at[2])
    arrived(CA.at[pl.ds(0, 3)], inn.at[CS])
    arrived(FULL.at[0, 0], inn.at[DDUP])
    mixed = jnp.zeros((192, 128), f32)
    for b in range(N):
        mixed += jnp.dot(xv[:, b * 256 : (b + 1) * 256], assemble(FULL, x, b), preferred_element_type=f32)
    high, low = two_pieces(mixed)
    pieces = jnp.concatenate([high.T, low.T], axis=0)
    for b in range(4):
        product = jnp.dot(pieces, CA[b], preferred_element_type=f32)
        PB[:, :, b] = (product[:128] + product[128:]).reshape(2, N, 8, 256)
        send(PB.at[1 - c, :, b], PR.at[:, b], 8, inn.at[PS], other)
    weights_step(1)

    arrived(PR, inn.at[PS])
    SB[...] = PB[c] + PR[...]
    for d in FAR_FIRST:
        send(SB.at[ring(f, d)], R1.at[f], 9, inn.at[B1], on_first(d))
    weights_step(2)
    arrived(R1.at[pl.ds(0, 7)], inn.at[B1])
    acc = SB[f]
    for d in FAR_FIRST:
        acc += R1[ring(f, -d)]
    S1[...] = acc

    for d in FAR_FIRST + (0,):
        for e in (2, 1, 3, 0):
            if d or e:
                send(S1.at[plane(e)], R2.at[x * N + s], 10, inn.at[B2], {**on_second(d), "tp": plane(e)})
    R2[x * N + s] = S1[x]
    weights_step(3)
    for d, h in ((1, 0), (3, 1)):
        arrived(FULL.at[0, 0], fx.at[d])
        same(FULL.at[plane(4 - d), c, pl.ds(4 * h, 4)], 16, fx.at[0], {"tp": plane(d)})
        same(FULL.at[plane(4 - d), c], 15, inn.at[FD], other)
    arrived(MOM.at[pl.ds(0, 7)], inn.at[MS])
    for k in (0, 1):
        for m in (0, 1):
            for b in range(N):
                MF[k, m, b // 4, 2 * (b % 4) : 2 * (b % 4) + 2, :] = MOM[b, k, m]

    arrived(R2.at[pl.ds(0, 31)], inn.at[B2])
    sums = []
    for k in (0, 1):
        squares = 0.0
        for h in (0, 1):
            at = (2 * k + h) * N
            small = R2[at]
            for b in range(1, N):
                small += R2[at + b]
            first_new = beta_one * MF[k, 0, h] + (1.0 - beta_one) * small
            second_new = beta_two * MF[k, 1, h] + (1.0 - beta_two) * small * small
            direction = first_new / (jnp.sqrt(second_new) + denom_floor)
            DD[c, f, k, h] = direction
            squares += direction * direction
            T[k, 0, h] = first_new
            T[k, 1, h] = second_new
        sums.append(jnp.sum(squares, axis=(0, 1), keepdims=True))
    for d in FAR_FIRST:
        same(DD.at[c, f], 11, c1.at[d], on_first(d))
    same(DD.at[c, f], 12, inn.at[CD], other)

    row = lax.broadcasted_iota(jnp.int32, (2, 128), 0)
    mine = (c * N + f) * 4 + x
    TS[mine] = jnp.where(row == 0, sums[0], sums[1])
    for d in FAR_FIRST + (0,):
        for e in (2, 1, 3, 0):
            for core in (c, 1 - c):
                if d or e or core is not c:
                    same(TS.at[mine], 13, inn.at[TSUM], {**on_first(d), "tp": plane(e), "c": core})
    weights_step(4)
    for k in (0, 1):
        for m in (0, 1):
            for b in range(N):
                M8[k, m, b] = T[k, m, b // 4, 2 * (b % 4) : 2 * (b % 4) + 2, :]
            mom_ref[k, m] = M8[k, m, s]
    for d in FAR_FIRST:
        arrived(DD.at[0, 0], c1.at[d])
        same(DD.at[c, ring(f, -d)], 12, inn.at[CD], other)
    arrived(FULL.at[0, 0], fx.at[0])
    same(FULL.at[plane(2), c], 15, inn.at[FD], other)
    arrived(TS.at[pl.ds(0, 63)], inn.at[TSUM])
    total = TS[0]
    for b in range(1, 64):
        total += TS[b]
    line = lax.broadcasted_iota(jnp.int32, (8, 256), 0)
    total_ref[...] = jnp.where(line == 0, total[0:1, 0:1], total[1:2, 0:1])
    arrived(DD.at[0], inn.at[CD])
    arrived(FULL.at[pl.ds(0, 3), 0], inn.at[FD])
    for k, p in both:
        arrived(p.one_core(W[k]), wd.at[k])

    for group, view in enumerate((
        FULL.at[0, 0, 0, pl.ds(0, 7)], FULL.at[0, 0, pl.ds(0, 7)], FULL.at[0, 0], MOM.at[pl.ds(0, 7)],
        CA.at[pl.ds(0, 3)], WQ.at[pl.ds(0, 7), 0, :, 0], WQ.at[pl.ds(0, 7)], WQ, PB.at[0], R1.at[pl.ds(0, 7)],
        R2.at[pl.ds(0, 31)], DD.at[0, pl.ds(0, 7)], DD.at[0], TS.at[pl.ds(0, 63)],
        FULL.at[pl.ds(0, 2), 0], FULL.at[pl.ds(0, 3), 0], FULL.at[0, 0],
    )):
        arrived(view, out.at[group])


def update_kernel(
    FULL, WQ, WK, DD, total_ref, mom_ref,
    uq_out, nq_out, cq_out, f1q_out, f2q_out, uk_out, nk_out, ck_out, f1k_out, f2k_out,
    copies, own, mom, sems, small_sems,
):
    z, y, c = (lax.axis_index(a) for a in FS)
    f, s = jnp.where(c == 0, y, z), jnp.where(c == 0, z, y)
    W = (WQ, WK)
    outs = ((uq_out, nq_out, cq_out, f1q_out, f2q_out), (uk_out, nk_out, ck_out, f1k_out, f2k_out))
    flight = []
    mom[...] = mom_ref[...]
    for k in (0, 1):
        for m in (0, 1):
            copy = pltpu.make_async_copy(mom.at[k, m], outs[k][3 + m], small_sems.at[k, m])
            copy.start()
            flight.append(copy)
    for k in (0, 1):
        total = total_ref[k : k + 1, :]
        scale = 1.0 / jnp.maximum(jnp.sqrt(total * (1.0 / 262144.0)), scale_floor)
        full = jnp.concatenate([DD[:, :, k, h].reshape(128, 256) for h in (0, 1)], axis=0)
        high, low = two_pieces(full)

        def update_of(rows):
            whole = jnp.dot(rows, high, preferred_element_type=f32) + jnp.dot(rows, low, preferred_element_type=f32)
            return -scale * whole

        for b in range(N):
            rows = jnp.concatenate([assemble(FULL, 2 * k, b), assemble(FULL, 2 * k + 1, b)], axis=1)
            new = rows_of(W[k], k, b) + learn_rate * update_of(rows)
            copies[k, b] = new.astype(bf16)
            copy = pltpu.make_async_copy(copies.at[k, b], outs[k][2].at[pl.ds(b * 256, 256), :], sems.at[k, b])
            copy.start()
            flight.append(copy)
        update = update_of(jnp.concatenate([FULL[2 * k, c, s, f], FULL[2 * k + 1, c, s, f]], axis=1))
        own[k, 0] = update
        own[k, 1] = own_rows(W[k], k, z, y, c) + learn_rate * update
        for m in (0, 1):
            copy = pltpu.make_async_copy(own.at[k, m], outs[k][m], small_sems.at[k, 2 + m])
            copy.start()
            flight.append(copy)
    for copy in flight:
        copy.wait()


def body(*args):
    hbm = pl.BlockSpec(memory_space=pltpu.HBM)
    vmem = pl.BlockSpec(memory_space=pltpu.VMEM)
    shape = jax.ShapeDtypeStruct
    by_z, by_y = (8, 4, 2, 2, 16, 256), (4, 2, 8, 2, 16, 256)
    dma = pltpu.SemaphoreType.DMA
    room = pltpu.VMEM
    mid = pl.pallas_call(
        exchange_kernel,
        out_shape=(
            room((4, 2, 8, 8, 16, 128), bf16), room(by_z, f32), room(by_y, f32),
            room((2, 8, 2, 2, 8, 256), f32), room((8, 256), f32), room((2, 2, 2, 256), f32),
        ),
        in_specs=[hbm] * 11,
        out_specs=(vmem,) * 6,
        scratch_shapes=[
            room((192, 2048), bf16), room((2, 192, 256), bf16), room((4, 192, 256), bf16), room((2, 16, 256), bf16),
            room((8, 2, 2, 2, 256), f32), room((2, 2, 2, 8, 256), f32),
            room((2, 8, 4, 8, 256), f32), room((8, 4, 8, 256), f32), room((8, 4, 8, 256), f32), room((8, 4, 8, 256), f32),
            room((4, 8, 256), f32), room((32, 8, 256), f32), room((64, 2, 128), f32),
            room((2, 2, 2, 8, 256), f32), room((2, 2, 8, 2, 256), f32),
            dma((6,)), dma((17,)), dma((10,)), dma((4,)), dma((8,)), dma((8,)), dma((2,)), dma((2, 4)), dma((2, 4)), dma((2,)),
        ],
        compiler_params=pltpu.CompilerParams(collective_id=0, has_side_effects=True, vmem_limit_bytes=40 * 1024 * 1024),
    )(*(pltpu.with_memory_space_constraint(a, pltpu.HBM) for a in args))
    one = (
        shape((16, 256), f32), shape((16, 256), f32), shape((2048, 256), bf16), shape((2, 256), f32), shape((2, 256), f32),
    )
    return pl.pallas_call(
        update_kernel,
        out_shape=one + one,
        in_specs=[vmem] * 6,
        out_specs=(hbm,) * 10,
        scratch_shapes=[
            room((2, 8, 256, 256), bf16), room((2, 2, 16, 256), f32), room((2, 2, 2, 256), f32), dma((2, 8)), dma((2, 4)),
        ],
        compiler_params=pltpu.CompilerParams(vmem_limit_bytes=40 * 1024 * 1024),
    )(*mid)


def solution(mesh):
    split = Mesh(mesh.devices.reshape(8, 8, 2, mesh.shape["tp"]), ("z", "y", "c", "tp"))
    rows, tiles = P(FS, None), P(FS, "tp")
    one = (tiles, tiles, P(None, "tp"), tiles, tiles)
    return jax.shard_map(
        body,
        mesh=split,
        in_specs=(rows, tiles, tiles, rows, rows, tiles, tiles, tiles, tiles, tiles, tiles),
        out_specs=one + one,
        check_vma=False,
    )
```
